32 devices in a mesh: rep: 4 (over z), fs: 4 (over y, x), tp: 2 (over core).
Axes of the slice: x: 2, y: 2, z: 4, core: 2. Of those that a mesh axis runs over, the one named last changes fastest.
Arguments:
- tokens: bfloat16 [16, 768, 2048], P(('rep', 'fs')), may hold values from -6 to 6
- norm_gain: float32 [2048], replicated, may hold values from 0.1 to 1.9
- outer_weight: bfloat16 [2048, 2048], P('fs', 'tp'), may hold values from -0.125 to 0.125
- inner_weight: bfloat16 [2048, 2048], P('fs', 'tp'), may hold values from -0.125 to 0.125
- value_weight: bfloat16 [2048, 2048], P('fs', 'tp'), may hold values from -0.125 to 0.125
- conv_taps: float32 [3, 2048], replicated, may hold values from -3.5 to 3.5
- out_weight: bfloat16 [2048, 2048], P('fs', 'tp'), may hold values from -0.125 to 0.125
Outputs:
- mixed: bfloat16 [16, 768, 2048], P(('rep', 'fs'), None, 'tp')
The draws below stay inside these ranges and needn't reach their ends.
All inputs are finite; a program needn't handle non-finite values.
Results may differ from the reference program's by a relative error of at most 0.014.
Values may be sent and summed in bfloat16 or wider, within the bound.
A program may use at most 64 MiB of HBM per device.

```python
import jax
import jax.numpy as jnp
from jax import lax

D = 2048
TAPS = 3
SEQ = 768
BATCH = 16


def steps_of(rng, dims, cuts, least, top_value):
    level = 1.0
    for axis_at, parts in cuts:
        heights = jax.random.uniform(jax.random.fold_in(jax.random.fold_in(rng, 6), axis_at), (parts,), jnp.float32, least / len(cuts), top_value / len(cuts))
        level = level * jnp.repeat(jnp.exp(heights), dims[axis_at] // parts).reshape((-1,) + (1,) * (len(dims) - 1 - axis_at))
    return level


def bell_draw(key, extent, deviation, limit, cuts=(), kind=jnp.bfloat16):
    array = deviation * jax.random.normal(key, extent, jnp.float32)
    if cuts:
        array = array * steps_of(key, extent, cuts, -0.22, 0.18)
    return jnp.clip(array, -limit, limit).astype(kind)


def setup_inputs(seed: int = 0) -> dict:
    seeds = jax.random.split(jax.random.key(seed), 8)
    tokens = bell_draw(seeds[0], (BATCH, SEQ, D), 1.0, 6.0, ((0, 16),))
    norm_gain = jnp.clip(1.0 + 0.18 * jax.random.normal(seeds[1], (D,), jnp.float32), 0.1, 1.9)
    outer_weight = bell_draw(seeds[2], (D, D), D ** -0.5, 0.125, ((0, 4), (1, 2)))
    inner_weight = bell_draw(seeds[3], (D, D), D ** -0.5, 0.125, ((0, 4), (1, 2)))
    value_weight = bell_draw(seeds[4], (D, D), D ** -0.5, 0.125, ((0, 4), (1, 2)))
    conv_taps = bell_draw(seeds[5], (TAPS, D), TAPS ** -0.5, 3.5, (), jnp.float32)
    out_weight = bell_draw(seeds[6], (D, D), D ** -0.5, 0.125, ((0, 4), (1, 2)))
    return {"tokens": tokens, "norm_gain": norm_gain, "outer_weight": outer_weight, "inner_weight": inner_weight, "value_weight": value_weight, "conv_taps": conv_taps, "out_weight": out_weight}


def reference(tokens, norm_gain, outer_weight, inner_weight, value_weight, conv_taps, out_weight):
    xf = tokens.astype(jnp.float32)
    scale = lax.rsqrt(lax.optimization_barrier(jnp.mean(xf * xf, axis=-1, keepdims=True)) + 1e-06)
    normed = (xf * scale * norm_gain).astype(jnp.bfloat16)
    rows = normed.reshape(BATCH * SEQ, D)
    outer = jnp.dot(rows, outer_weight, preferred_element_type=jnp.float32).astype(jnp.bfloat16)
    inner = jnp.dot(rows, inner_weight, preferred_element_type=jnp.float32).astype(jnp.bfloat16)
    value = jnp.dot(rows, value_weight, preferred_element_type=jnp.float32).astype(jnp.bfloat16)
    product = (inner.astype(jnp.float32) * value.astype(jnp.float32)).reshape(BATCH, SEQ, D)
    padded = jnp.pad(product, ((0, 0), (TAPS - 1, 0), (0, 0)))
    convolved = jnp.zeros((BATCH, SEQ, D), jnp.float32)
    for k in range(TAPS):
        convolved = convolved + conv_taps[k] * padded[:, k:k + SEQ, :]
    gated = (outer.astype(jnp.float32) * convolved.reshape(BATCH * SEQ, D)).astype(jnp.bfloat16)
    total = jnp.dot(gated, out_weight, preferred_element_type=jnp.float32)
    return total.astype(jnp.bfloat16).reshape(BATCH, SEQ, D)
```

```python
import jax
import jax.numpy as jnp
from jax import lax
from jax.experimental import pallas as pl
from jax.experimental.pallas import tpu as pltpu
from jax.sharding import PartitionSpec as P

MESH = pl.DeviceIdType.MESH
F32 = jnp.float32
BF16 = jnp.bfloat16


def plain(tokens, norm_gain, outer_weight, inner_weight, value_weight, conv_taps, out_weight):
    batch, seq_len, width = tokens.shape
    xf = tokens.astype(F32)
    scale = lax.rsqrt(jnp.mean(xf * xf, axis=-1, keepdims=True) + 1e-06)
    normed = (xf * scale * norm_gain).astype(BF16).reshape(batch * seq_len, width)
    columns = outer_weight.shape[1]

    def project(weight):
        full = lax.all_gather(weight, "fs", axis=0, tiled=True)
        return jnp.dot(normed, full, preferred_element_type=F32).astype(BF16).astype(F32)

    outer, inner, value = project(outer_weight), project(inner_weight), project(value_weight)
    product = (inner * value).reshape(batch, seq_len, columns)
    offset = lax.axis_index("tp") * columns
    taps = lax.dynamic_slice_in_dim(conv_taps, offset, columns, 1)
    count = conv_taps.shape[0]
    padded = jnp.pad(product, ((0, 0), (count - 1, 0), (0, 0)))
    convolved = jnp.zeros((batch, seq_len, columns), F32)
    for k in range(count):
        convolved = convolved + taps[k] * padded[:, k : k + seq_len, :]
    gated = (outer * convolved.reshape(batch * seq_len, columns)).astype(BF16)
    everything = lax.all_gather(gated, "tp", axis=1, tiled=True)
    full = lax.all_gather(out_weight, "fs", axis=0, tiled=True)
    result = jnp.dot(everything, full, preferred_element_type=F32)
    return result.astype(BF16).reshape(batch, seq_len, columns)


PARTS = 4
PAD = 16
COPIES = 112


def kernel(
    tok_hbm, gain_ref, outer_hbm, inner_hbm, value_hbm, taps_ref, outw_hbm, out_ref,
    tok, nm, wts, outw, proj, gat, mine, osum, send_sems, recv_sems, local_sems,
):
    rep, fs, tp = lax.axis_index("rep"), lax.axis_index("fs"), lax.axis_index("tp")
    seq, width = tok_hbm.shape
    rows, cols = outer_hbm.shape
    part = cols // PARTS
    hseq = seq // 2
    hrows = rows // 2
    qrows = rows // 4
    count = taps_ref.shape[0]
    m = rep // 2
    inner_chip = lax.rem(rep, 2) + m - 2 * lax.rem(rep, 2) * m
    fx = fs + 1 - 2 * lax.rem(fs, 2)
    fy = lax.rem(fs + 2, 4)
    fd = 3 - fs
    fp = fy + m * (fx - fy)
    fq = fx + m * (fy - fx)
    to_x, to_y, to_p, to_q = (rep, fx, tp), (rep, fy, tp), (rep, fp, tp), (rep, fq, tp)
    to_z, to_t = (rep + 1 - 2 * lax.rem(rep, 2), fs, tp), (rep, fs, 1 - tp)
    to_m = (3 - rep, fs, tp)
    keys = {}

    barrier = pltpu.get_barrier_semaphore()
    for peer in (to_x, to_y, to_z, to_t):
        pl.semaphore_signal(barrier, inc=1, device_id=peer, device_id_type=MESH)

    hbm = (inner_hbm, value_hbm, outer_hbm)
    tok_load = pltpu.make_async_copy(tok_hbm, tok.at[0], local_sems.at[0])
    tok_load.start()

    def al(x, n):
        return pl.multiple_of(x, n)

    tile = 128

    def norm(s, h, halves):
        @pl.loop(0, halves * hseq // tile)
        def _(b):
            r = al(h * hseq + b * tile, tile)
            xf = tok[s, pl.ds(r, tile), :].astype(F32)
            scale = lax.rsqrt(jnp.mean(xf * xf, axis=-1, keepdims=True) + 1e-06)
            nm[pl.ds(al(s * seq + r, tile), tile), :] = (xf * scale * gain_ref[...]).astype(BF16)

    zeros = jnp.zeros((PAD, part), BF16)
    for c in range(PARTS - 1):
        for w in range(2):
            for s in range(2):
                proj[w, c, s, 0:PAD, :] = zeros

    def project(units, blocks):
        b0, nb = blocks[0], len(blocks)
        u0, nu = units[0], len(units)

        @pl.loop(0, nu * nb)
        def _(i):
            u = u0 + i // nb
            b = b0 + lax.rem(i, nb)
            s, h = b // 2, lax.rem(b, 2)
            d = jnp.dot(nm[pl.ds(al(b * hseq, 128), hseq), :], wts[u], preferred_element_type=F32)
            proj[lax.rem(u, 3), u // 3, s, pl.ds(al(PAD + h * hseq, PAD), hseq), :] = d.astype(BF16)

    def gate(c, first, s, h, halves, store):
        tcols = pl.ds(al(tp * cols + first + c * part, 128), part)

        @pl.loop(0, halves * hseq // tile)
        def _(b):
            r = al(h * hseq + b * tile, tile)
            inner = proj[0, c, s, pl.ds(r, tile + PAD), :].astype(F32)
            value = proj[1, c, s, pl.ds(r, tile + PAD), :].astype(F32)
            outer = proj[2, c, s, pl.ds(al(r + PAD, PAD), tile), :].astype(F32)
            window = inner * value
            conv = jnp.zeros((tile, part), F32)
            for k in range(count):
                lo = PAD - (count - 1) + k
                conv = conv + taps_ref[k : k + 1, tcols] * window[lo : lo + tile, :]
            store(pl.ds(r, tile), (outer * conv).astype(BF16))

    def mix(tile_rows, b0, nb, terms, first, last):
        @pl.loop(b0, b0 + nb)
        def _(b):
            r = pl.ds(al(b * tile_rows, tile_rows), tile_rows)
            total = None
            for k, n in terms:
                d = jnp.dot(gat[r, pl.ds(k, n)], outw[pl.ds(k, n), :], preferred_element_type=F32)
                total = d if total is None else total + d
            if not first:
                total = total + osum[r, :]
            if last:
                out_ref[r, :] = total.astype(BF16)
            else:
                osum[r, :] = total

    def program(inside):
        sent = []

        def index(key):
            return keys.setdefault(key, len(keys))

        def send(key, src, dst, device):
            k = index(key)
            copy = pltpu.make_async_remote_copy(
                src_ref=src, dst_ref=dst, send_sem=send_sems.at[k], recv_sem=recv_sems.at[k],
                device_id=device, device_id_type=MESH,
            )
            copy.start()
            sent.append(copy)

        def wait(key, dst):
            k = index(key)
            pltpu.make_async_remote_copy(
                src_ref=dst, dst_ref=dst, send_sem=send_sems.at[k], recv_sem=recv_sems.at[k],
                device_id=to_t, device_id_type=MESH,
            ).wait_recv()

        chunks = PARTS - 1 if inside else 1
        first = part if inside else 0
        other_chunks = PARTS - chunks
        other_first = 0 if inside else part
        units = 3 * chunks
        w_load = []
        for u in range(units):
            c, w = u // 3, u % 3
            w_load.append(pltpu.make_async_copy(
                hbm[w].at[:, pl.ds(first + c * part, part)],
                wts.at[u, pl.ds(al(fs * rows, rows), rows)], local_sems.at[2 + u],
            ))
            w_load[u].start()
        ow_load = pltpu.make_async_copy(
            outw_hbm, outw.at[pl.ds(al(fs * rows, rows), rows)], local_sems.at[1])
        ow_load.start()

        def wrow(u, f, off, n):
            return wts.at[u, pl.ds(al(f * rows + off, 128), n)]

        def orow(f, off, n):
            return outw.at[pl.ds(al(f * rows + off, 128), n)]

        def trow(h, t):
            return pl.ds(al(h * hseq + t * (hseq // 2), 64), hseq // 2)

        def tok_z(h):
            send(("tz", h), tok_hbm.at[trow(h, tp)], tok.at[1, trow(h, tp)], to_z)

        def tok_f(h):
            here = tok.at[1, trow(h, tp)]
            wait(("tz", h), here)
            send(("tt", h), here, here, to_t)

        def tok_w(h):
            wait(("tt", h), tok.at[1, trow(h, 1 - tp)])

        def gcols(t, base, c):
            return pl.ds(al(t * cols + base + c * part, 128), part)

        def grow(h):
            return pl.ds(h * hseq, hseq)

        def own_gate(c, finish=True):
            def store(r, x):
                gat[r, gcols(tp, first, c)] = x
            gate(c, first, 0, 0, 2, store)
            here = gat.at[:, gcols(tp, first, c)]
            send(("gt", c, inside), here, here, to_t)

        def partner_gate(c, h):
            def store(r, x):
                mine[c, r, :] = x
            gate(c, first, 1, h, 1, store)
            send(("gz", c, h, inside), mine.at[c, grow(h)], gat.at[grow(h), gcols(tp, first, c)], to_z)

        def take(c, h):
            here = gat.at[grow(h), gcols(tp, other_first, c)]
            wait(("gz", c, h, not inside), here)
            send(("gf", c, h, inside), here, here, to_t)

        def own_other(c):
            wait(("gt", c, inside), gat.at[:, gcols(1 - tp, first, c)])

        def take_other(c, h):
            wait(("gf", c, h, inside), gat.at[grow(h), gcols(1 - tp, other_first, c)])

        f_off, g_off, c_off = m * hrows, (1 - m) * hrows, (1 - m) * 3 * qrows

        if inside:
            pl.semaphore_signal(barrier, inc=1, device_id=to_m, device_id_type=MESH)
            pl.semaphore_wait(barrier, 5)
            hx, hy = m * hrows, (1 - m) * hrows
            woff = m * qrows

            def direct(u):
                c, w = u // 3, u % 3
                at = pl.ds(first + c * part, part)
                send(("dx", u), hbm[w].at[pl.ds(al(hx, 128), hrows), at], wrow(u, fs, hx, hrows), to_x)
                send(("dy", u), hbm[w].at[pl.ds(al(hy, 128), hrows), at], wrow(u, fs, hy, hrows), to_y)

            def relay(u):
                wait(("dx", u), wrow(u, fx, hx, hrows))
                wait(("dy", u), wrow(u, fy, hy, hrows))
                bx, by = wrow(u, fx, hx, hrows), wrow(u, fy, hy, hrows)
                send(("mx", u), bx, bx, to_m)
                send(("rx", u), by, by, to_x)
                send(("ry", u), bx, bx, to_y)
                send(("my", u), by, by, to_m)

            def ready(u):
                w_load[u].wait()
                wait(("rx", u), wrow(u, fd, hy, hrows))
                wait(("ry", u), wrow(u, fd, hx, hrows))
                wait(("mx", u), wrow(u, fx, hrows - hx, hrows))
                wait(("my", u), wrow(u, fy, hrows - hy, hrows))

            tok_z(0)
            tok_z(1)
            for u in range(3):
                direct(u)
            tok_load.wait()
            norm(0, 0, 2)
            relay(0)
            direct(3)
            relay(1)
            direct(4)
            relay(2)
            direct(5)
            ready(0)
            project([0], [0, 1])
            relay(3)
            direct(6)
            ready(1)
            project([1], [0, 1])
            tok_f(0)
            relay(4)
            direct(7)
            tok_w(0)
            norm(1, 0, 1)
            ready(2)
            project([2], [0, 1])
            project([0, 1, 2], [2])
            partner_gate(0, 0)
            own_gate(0)
            relay(5)
            direct(8)
            ready(3)
            project([3], [0, 1, 2])
            relay(6)
            ready(4)
            project([4], [0, 1, 2])
            tok_f(1)
            relay(7)
            tok_w(1)
            norm(1, 1, 1)
            project([0, 1, 2], [3])
            partner_gate(0, 1)
            relay(8)
            for b in range(3):
                off = woff + b * qrows
                src = outw_hbm.at[pl.ds(al(off, 128), qrows)]
                send(("ox", b), src, orow(fs, off, qrows), to_x)
                send(("oy", b), src, orow(fs, off, qrows), to_y)
            ready(5)
            project([5], [0, 1, 2])
            partner_gate(1, 0)
            project([3, 4, 5], [3])
            partner_gate(1, 1)
            own_gate(1)
            block = orow(fd, f_off, hrows)
            wait(("oz", 0), block)
            send(("om",), block, block, to_m)
            ready(6)
            project([6], [0, 1, 2, 3])
            ready(7)
            project([7], [0, 1, 2, 3])
            ready(8)
            project([8], [2])
            partner_gate(2, 0)
            project([8], [3])
            partner_gate(2, 1)
            project([8], [0, 1])
            own_gate(2)
            for h in range(2):
                take(0, h)
            ow_load.wait()
            for c in range(chunks):
                own_other(c)
            for h in range(2):
                take_other(0, h)
            big = hseq
            mix(big, 0, 2, [(al(fs * rows, rows), rows), (al(fd * rows + f_off, 128), hrows)], True, False)
            for b in range(2):
                off = woff + b * qrows
                wait(("ox", b), orow(fx, off, qrows))
                wait(("oy", b), orow(fy, off, qrows))
            mix(big, 0, 2, [(al(f * rows + woff, 128), hrows) for f in (fx, fy)], False, False)
            wait(("oz", 1), orow(fq, c_off, qrows))
            wait(("oz", 2), orow(fp, c_off, qrows))
            wait(("om",), orow(fd, g_off, hrows))
            mix(big, 0, 2, [(al(f * rows + c_off, 128), qrows) for f in (fx, fy)]
                + [(al(fd * rows + g_off, 128), hrows)], False, False)
            off = woff + 2 * qrows
            wait(("ox", 2), orow(fx, off, qrows))
            wait(("oy", 2), orow(fy, off, qrows))
            mix(big, 0, 2, [(al(f * rows + off, 128), qrows) for f in (fx, fy)], False, True)
        else:
            pl.semaphore_wait(barrier, 4)

            def direct(u, which):
                c, w = u // 3, u % 3
                src = hbm[w].at[:, pl.ds(first + c * part, part)]
                send(("d" + which, u), src, wrow(u, fs, 0, rows), to_p if which == "p" else to_q)

            def relay_q(u):
                wait(("dp", u), wrow(u, fp, 0, rows))
                block = wrow(u, fp, f_off, hrows)
                send(("rq", u), block, block, to_q)

            def relay_p(u):
                wait(("dq", u), wrow(u, fq, 0, rows))
                block = wrow(u, fq, g_off, hrows)
                send(("rp", u), block, block, to_p)

            def ready(u):
                w_load[u].wait()
                wait(("rq", u), wrow(u, fd, f_off, hrows))
                wait(("rp", u), wrow(u, fd, g_off, hrows))

            def out_rows(off):
                return outw_hbm.at[pl.ds(al(off, 128), hrows)]

            tok_z(0)
            tok_z(1)
            send(("op", 0), out_rows(f_off), orow(fs, f_off, hrows), to_p)
            for u in range(3):
                direct(u, "q")
                direct(u, "p")
            tok_load.wait()
            norm(0, 0, 2)
            relay_p(0)
            relay_p(1)
            block = orow(fp, f_off, hrows)
            wait(("op", 0), block)
            send(("orq",), block, block, to_q)
            relay_p(2)
            send(("op", 1), out_rows(g_off), orow(fs, g_off, hrows), to_p)
            relay_q(0)
            tok_f(0)
            relay_q(1)
            tok_w(0)
            norm(1, 0, 1)
            relay_q(2)
            send(("oq", 0), out_rows(g_off), orow(fs, g_off, hrows), to_q)
            send(("oq", 1), out_rows(f_off), orow(fs, f_off, hrows), to_q)
            block = orow(fd, f_off, hrows)
            wait(("orq",), block)
            send(("oz", 0), block, block, to_z)
            for u in range(2):
                ready(u)
                project([u], [0, 1, 2])
            tok_f(1)
            ready(2)
            project([2], [2])
            partner_gate(0, 0)
            tok_w(1)
            norm(1, 1, 1)
            project([0, 1, 2], [3])
            partner_gate(0, 1)
            project([2], [0, 1])
            own_gate(0)
            wait(("op", 1), orow(fp, g_off, hrows))
            block = orow(fp, c_off, qrows)
            send(("oz", 2), block, block, to_z)
            block = orow(fq, g_off, hrows)
            wait(("oq", 0), block)
            send(("orp",), block, block, to_p)
            block = orow(fq, c_off, qrows)
            send(("oz", 1), block, block, to_z)
            own_other(0)
            for h in range(2):
                take(0, h)
            wait(("oq", 1), orow(fq, f_off, hrows))
            ow_load.wait()
            for h in range(2):
                take_other(0, h)
            for h in range(2):
                take(1, h)
            wait(("orp",), orow(fd, g_off, hrows))
            mix(hseq, 0, 2, [(0, 2 * part), (cols, 2 * part)], True, False)
            for h in range(2):
                take_other(1, h)
            mix(hseq, 0, 2, [(2 * part, part), (cols + 2 * part, part)], False, False)
            for h in range(2):
                take(2, h)
                take_other(2, h)
                mix(hseq, h, 1, [(3 * part, part), (cols + 3 * part, part)], False, True)

        for copy in sent:
            copy.wait_send()

    @pl.when(inner_chip == 1)
    def _():
        program(True)

    @pl.when(inner_chip == 0)
    def _():
        program(False)

    assert len(keys) <= COPIES


def paired(tokens, norm_gain, outer_weight, inner_weight, value_weight, conv_taps, out_weight):
    _, seq, width = tokens.shape
    rows, cols = outer_weight.shape
    part = cols // PARTS
    anyspace = pl.BlockSpec(memory_space=pltpu.HBM)
    vmem = pl.BlockSpec(memory_space=pltpu.VMEM)
    out = pl.pallas_call(
        kernel,
        out_shape=pltpu.VMEM((seq, cols), BF16),
        in_specs=[anyspace, vmem, anyspace, anyspace, anyspace, vmem, anyspace],
        out_specs=vmem,
        scratch_shapes=[
            pltpu.VMEM((2, seq, width), BF16),
            pltpu.VMEM((2 * seq, width), BF16),
            pltpu.VMEM((3 * (PARTS - 1), width, part), BF16),
            pltpu.VMEM((width, cols), BF16),
            pltpu.VMEM((3, PARTS - 1, 2, seq + PAD, part), BF16),
            pltpu.VMEM((seq, width), BF16),
            pltpu.VMEM((PARTS - 1, seq, part), BF16),
            pltpu.VMEM((seq, cols), F32),
            pltpu.SemaphoreType.DMA((COPIES,)),
            pltpu.SemaphoreType.DMA((COPIES,)),
            pltpu.SemaphoreType.DMA((2 + 3 * (PARTS - 1),)),
        ],
        compiler_params=pltpu.CompilerParams(
            collective_id=0, has_side_effects=True, vmem_limit_bytes=58 * 1024 * 1024
        ),
        name="mixer",
    )(
        tokens.reshape(seq, width), norm_gain.reshape(1, width), outer_weight, inner_weight,
        value_weight, conv_taps, out_weight,
    )
    return out.reshape(1, seq, cols)


def solution(mesh):
    shape = dict(mesh.shape)

    def local(tokens, *rest):
        rows, cols = rest[1].shape
        fits = (
            shape["fs"] == 4 and shape["tp"] == 2 and shape["rep"] == 4
            and tokens.shape[0] == 1 and tokens.shape[1] % 256 == 0
            and rows % 512 == 0 and cols == 2 * rows and rest[4].shape[0] <= 9
        )
        return (paired if fits else plain)(tokens, *rest)

    in_specs = (
        P(("rep", "fs"), None, None),
        P(),
        P("fs", "tp"),
        P("fs", "tp"),
        P("fs", "tp"),
        P(),
        P("fs", "tp"),
    )
    out_specs = P(("rep", "fs"), None, "tp")
    return jax.shard_map(local, mesh=mesh, in_specs=in_specs, out_specs=out_specs, check_vma=False)
```

```python
import jax
import jax.numpy as jnp
from jax import lax
from jax.experimental import pallas as pl
from jax.experimental.pallas import tpu as pltpu
from jax.sharding import PartitionSpec as P

MESH = pl.DeviceIdType.MESH
F32 = jnp.float32
BF16 = jnp.bfloat16


def plain(tokens, norm_gain, outer_weight, inner_weight, value_weight, conv_taps, out_weight):
    batch, seq_len, width = tokens.shape
    xf = tokens.astype(F32)
    scale = lax.rsqrt(jnp.mean(xf * xf, axis=-1, keepdims=True) + 1e-06)
    normed = (xf * scale * norm_gain).astype(BF16).reshape(batch * seq_len, width)
    columns = outer_weight.shape[1]

    def project(weight):
        full = lax.all_gather(weight, "fs", axis=0, tiled=True)
        return jnp.dot(normed, full, preferred_element_type=F32).astype(BF16).astype(F32)

    outer, inner, value = project(outer_weight), project(inner_weight), project(value_weight)
    product = (inner * value).reshape(batch, seq_len, columns)
    offset = lax.axis_index("tp") * columns
    taps = lax.dynamic_slice_in_dim(conv_taps, offset, columns, 1)
    count = conv_taps.shape[0]
    padded = jnp.pad(product, ((0, 0), (count - 1, 0), (0, 0)))
    convolved = jnp.zeros((batch, seq_len, columns), F32)
    for k in range(count):
        convolved = convolved + taps[k] * padded[:, k : k + seq_len, :]
    gated = (outer * convolved.reshape(batch * seq_len, columns)).astype(BF16)
    everything = lax.all_gather(gated, "tp", axis=1, tiled=True)
    full = lax.all_gather(out_weight, "fs", axis=0, tiled=True)
    result = jnp.dot(everything, full, preferred_element_type=F32)
    return result.astype(BF16).reshape(batch, seq_len, columns)


PARTS = 4
PAD = 16
CROSS = 9
COPIES = CROSS + 24


def kernel(
    tok_hbm, gain_hbm, outer_hbm, inner_hbm, value_hbm, taps_hbm, outw_hbm, out_ref,
    gain_ref, taps_ref, tok, nm, wts, outw, proj, gat, mine, osum, send_sems, recv_sems, local_sems,
):
    rep, fs, tp = lax.axis_index("rep"), lax.axis_index("fs"), lax.axis_index("tp")
    seq, width = tok_hbm.shape
    rows, cols = outer_hbm.shape
    part = cols // PARTS
    hseq = seq // 2
    hrows = rows // 2
    qrows = rows // 4
    count = taps_ref.shape[0]
    m = rep // 2
    inner_chip = lax.rem(rep, 2) + m - 2 * lax.rem(rep, 2) * m
    fx = fs + 1 - 2 * lax.rem(fs, 2)
    fy = lax.rem(fs + 2, 4)
    fd = 3 - fs
    fp = fy + m * (fx - fy)
    fq = fx + m * (fy - fx)
    to_x, to_y, to_p, to_q = (rep, fx, tp), (rep, fy, tp), (rep, fp, tp), (rep, fq, tp)
    to_z, to_t = (rep + 1 - 2 * lax.rem(rep, 2), fs, tp), (rep, fs, 1 - tp)
    to_m = (3 - rep, fs, tp)
    cross = {}

    barrier = pltpu.get_barrier_semaphore()
    for peer in (to_x, to_y, to_z, to_t):
        pl.semaphore_signal(barrier, inc=1, device_id=peer, device_id_type=MESH)

    hbm = (inner_hbm, value_hbm, outer_hbm)
    tok_load = pltpu.make_async_copy(tok_hbm, tok.at[0], local_sems.at[0])
    gain_load = pltpu.make_async_copy(gain_hbm, gain_ref, local_sems.at[1])
    taps_load = pltpu.make_async_copy(taps_hbm, taps_ref, local_sems.at[2])
    gain_load.start()
    taps_load.start()
    tok_load.start()

    def al(x, n):
        return pl.multiple_of(x, n)

    tile = 128

    def norm(s, h, halves):
        @pl.loop(0, halves * hseq // tile)
        def _(b):
            r = al(h * hseq + b * tile, tile)
            xf = tok[s, pl.ds(r, tile), :].astype(F32)
            scale = lax.rsqrt(jnp.mean(xf * xf, axis=-1, keepdims=True) + 1e-06)
            nm[pl.ds(al(s * seq + r, tile), tile), :] = (xf * scale * gain_ref[...]).astype(BF16)

    zeros = jnp.zeros((PAD, part), BF16)
    for c in range(PARTS - 1):
        for w in range(2):
            for s in range(2):
                proj[w, c, s, 0:PAD, :] = zeros

    def project(units, blocks):
        b0, nb = blocks[0], len(blocks)
        u0, nu = units[0], len(units)

        @pl.loop(0, nu * nb)
        def _(i):
            u = u0 + i // nb
            b = b0 + lax.rem(i, nb)
            s, h = b // 2, lax.rem(b, 2)
            d = jnp.dot(nm[pl.ds(al(b * hseq, 128), hseq), :], wts[u], preferred_element_type=F32)
            proj[lax.rem(u, 3), u // 3, s, pl.ds(al(PAD + h * hseq, PAD), hseq), :] = d.astype(BF16)

    def gate(c, first, s, h, halves, store):
        tcols = pl.ds(al(tp * cols + first + c * part, 128), part)

        @pl.loop(0, halves * hseq // tile)
        def _(b):
            r = al(h * hseq + b * tile, tile)
            inner = proj[0, c, s, pl.ds(r, tile + PAD), :].astype(F32)
            value = proj[1, c, s, pl.ds(r, tile + PAD), :].astype(F32)
            outer = proj[2, c, s, pl.ds(al(r + PAD, PAD), tile), :].astype(F32)
            window = inner * value
            conv = jnp.zeros((tile, part), F32)
            for k in range(count):
                lo = PAD - (count - 1) + k
                conv = conv + taps_ref[k : k + 1, tcols] * window[lo : lo + tile, :]
            store(pl.ds(r, tile), (outer * conv).astype(BF16))

    def mix(tile_rows, b0, nb, terms, first, last):
        @pl.loop(b0, b0 + nb)
        def _(b):
            r = pl.ds(al(b * tile_rows, tile_rows), tile_rows)
            total = None
            for k, n in terms:
                d = jnp.dot(gat[r, pl.ds(k, n)], outw[pl.ds(k, n), :], preferred_element_type=F32)
                total = d if total is None else total + d
            if not first:
                total = total + osum[r, :]
            if last:
                out_ref[r, :] = total.astype(BF16)
            else:
                osum[r, :] = total

    def program(inside):
        local = {}

        def index(key):
            if key[0] in ("tz", "gz", "oz"):
                return cross.setdefault(key, len(cross))
            return CROSS + local.setdefault(key, len(local))

        def send(key, src, dst, device, group):
            k = index(key)
            pltpu.make_async_remote_copy(
                src_ref=src, dst_ref=dst, send_sem=send_sems.at[group], recv_sem=recv_sems.at[k],
                device_id=device, device_id_type=MESH,
            ).start()

        def wait(key, dst):
            k = index(key)
            pltpu.make_async_remote_copy(
                src_ref=dst, dst_ref=dst, send_sem=send_sems.at[0], recv_sem=recv_sems.at[k],
                device_id=to_t, device_id_type=MESH,
            ).wait_recv()

        def wait_sent(group, src):
            pltpu.make_async_remote_copy(
                src_ref=src, dst_ref=src, send_sem=send_sems.at[group], recv_sem=recv_sems.at[0],
                device_id=to_t, device_id_type=MESH,
            ).wait_send()

        chunks = PARTS - 1 if inside else 1
        first = part if inside else 0
        other_chunks = PARTS - chunks
        other_first = 0 if inside else part
        units = 3 * chunks
        for u in range(units):
            c, w = u // 3, u % 3
            pltpu.make_async_copy(
                hbm[w].at[:, pl.ds(first + c * part, part)],
                wts.at[u, pl.ds(al(fs * rows, rows), rows)], local_sems.at[3],
            ).start()
        w_load = pltpu.make_async_copy(
            wts.at[0:units, 0:rows], wts.at[0:units, 0:rows], local_sems.at[3])
        ow_load = pltpu.make_async_copy(
            outw_hbm, outw.at[pl.ds(al(fs * rows, rows), rows)], local_sems.at[4])
        ow_load.start()

        def wrow(u, f, off, n):
            return wts.at[u, pl.ds(al(f * rows + off, 128), n)]

        def orow(f, off, n):
            return outw.at[pl.ds(al(f * rows + off, 128), n)]

        def trow(h, t):
            return pl.ds(al(h * hseq + t * (hseq // 2), 64), hseq // 2)

        def tok_z(h):
            send(("tz", h), tok_hbm.at[trow(h, tp)], tok.at[1, trow(h, tp)], to_z, 1)

        def tok_f(h):
            here = tok.at[1, trow(h, tp)]
            wait(("tz", h), here)
            send(("tt", h), here, here, to_t, 1)

        def tok_w(h):
            wait(("tt", h), tok.at[1, trow(h, 1 - tp)])

        def gcols(t, base, c):
            return pl.ds(al(t * cols + base + c * part, 128), part)

        def grow(h):
            return pl.ds(0, seq) if h is None else pl.ds(h * hseq, hseq)

        def z_key(c, h, from_inside):
            return ("gz", c, h if from_inside and c == PARTS - 2 else None, from_inside)

        def own_gate(c, key):
            def store(r, x):
                gat[r, gcols(tp, first, c)] = x
            gate(c, first, 0, 0, 2, store)
            here = gat.at[:, gcols(tp, first, c)]
            send(key, here, here, to_t, 3)

        def partner_gate(c, h):
            def store(r, x):
                mine[c, r, :] = x
            gate(c, first, 1, h or 0, 2 if h is None else 1, store)
            send(z_key(c, h, inside), mine.at[c, grow(h)], gat.at[grow(h), gcols(tp, first, c)], to_z, 3)

        def take(c, h, key):
            here = gat.at[grow(h), gcols(tp, other_first, c)]
            wait(z_key(c, h, not inside), here)
            send(key, here, here, to_t, 3)

        def take_other(key, h, parts):
            wait(key, gat.at[grow(h), pl.ds(0, parts * part)])

        f_off, g_off, c_off = m * hrows, (1 - m) * hrows, (1 - m) * 3 * qrows

        if inside:
            pl.semaphore_signal(barrier, inc=1, device_id=to_m, device_id_type=MESH)
            pl.semaphore_wait(barrier, 5)
            hx, hy = m * hrows, (1 - m) * hrows
            woff = m * qrows

            def direct(u):
                c, w = u // 3, u % 3
                at = pl.ds(first + c * part, part)
                send(("d", u), hbm[w].at[pl.ds(al(hx, 128), hrows), at], wrow(u, fs, hx, hrows), to_x, 0)
                send(("d", u), hbm[w].at[pl.ds(al(hy, 128), hrows), at], wrow(u, fs, hy, hrows), to_y, 0)

            def relay(u):
                wait(("d", u), wts.at[u, 0 : 2 * hrows])
                bx, by = wrow(u, fx, hx, hrows), wrow(u, fy, hy, hrows)
                send(("r", u), bx, bx, to_m, 0)
                send(("r", u), by, by, to_x, 0)
                send(("r", u), bx, bx, to_y, 0)
                send(("r", u), by, by, to_m, 0)

            def ready(u):
                if u == 0:
                    w_load.wait()
                wait(("r", u), wts.at[u, 0 : 4 * hrows])

            tok_z(0)
            tok_z(1)
            for u in range(3):
                direct(u)
            tok_load.wait()
            gain_load.wait()
            norm(0, 0, 2)
            relay(0)
            direct(3)
            relay(1)
            direct(4)
            relay(2)
            direct(5)
            ready(0)
            project([0], [0, 1])
            relay(3)
            direct(6)
            ready(1)
            project([1], [0, 1])
            tok_f(0)
            relay(4)
            direct(7)
            tok_w(0)
            norm(1, 0, 1)
            ready(2)
            project([2], [0, 1])
            project([0, 1, 2], [2])
            taps_load.wait()
            partner_gate(0, 0)
            own_gate(0, ("ga",))
            relay(5)
            direct(8)
            ready(3)
            project([3], [0, 1, 2])
            relay(6)
            ready(4)
            project([4], [0, 1, 2])
            tok_f(1)
            relay(7)
            tok_w(1)
            norm(1, 1, 1)
            project([0, 1, 2], [3])
            partner_gate(0, 1)
            relay(8)
            for b in range(3):
                off = woff + b * qrows
                src = outw_hbm.at[pl.ds(al(off, 128), qrows)]
                send(("o", b), src, orow(fs, off, qrows), to_x, 2)
                send(("o", b), src, orow(fs, off, qrows), to_y, 2)
            ready(5)
            project([5], [0, 1, 2])
            partner_gate(1, 0)
            project([3, 4, 5], [3])
            partner_gate(1, 1)
            own_gate(1, ("ga",))
            block = orow(fd, f_off, hrows)
            wait(("oz", 0), block)
            send(("oz", 1), block, block, to_m, 2)
            ready(6)
            project([6], [0, 1, 2, 3])
            ready(7)
            project([7], [0, 1, 2, 3])
            ready(8)
            project([8], [2])
            partner_gate(2, 0)
            project([8], [3])
            partner_gate(2, 1)
            project([8], [0, 1])
            own_gate(2, ("ga",))
            take(0, None, ("ga",))
            ow_load.wait()
            take_other(("ga",), None, PARTS)
            big = hseq
            mix(big, 0, 2, [(al(fs * rows, rows), rows), (al(fd * rows + f_off, 128), hrows)], True, False)
            for b in range(2):
                wait(("o", b), outw.at[0 : 2 * qrows])
            mix(big, 0, 2, [(al(f * rows + woff, 128), hrows) for f in (fx, fy)], False, False)
            wait(("oz", 1), outw.at[0 : 4 * qrows])
            mix(big, 0, 2, [(al(f * rows + c_off, 128), qrows) for f in (fx, fy)]
                + [(al(fd * rows + g_off, 128), hrows)], False, False)
            off = woff + 2 * qrows
            wait(("o", 2), outw.at[0 : 2 * qrows])
            mix(big, 0, 2, [(al(f * rows + off, 128), qrows) for f in (fx, fy)], False, True)
            wait_sent(0, wts.at[:, 0 : 6 * hrows])
            wait_sent(1, tok.at[0])
            wait_sent(2, outw.at[0 : 8 * qrows])
            wait_sent(3, gat.at[:, 0 : 7 * part])
        else:
            pl.semaphore_wait(barrier, 4)

            def direct(u, which):
                c, w = u // 3, u % 3
                src = hbm[w].at[:, pl.ds(first + c * part, part)]
                send(("d" + which, u), src, wrow(u, fs, 0, rows), to_p if which == "p" else to_q, 0)

            def relay_q(u):
                wait(("dp", u), wrow(u, fp, 0, rows))
                block = wrow(u, fp, f_off, hrows)
                send(("r", u), block, block, to_q, 0)

            def relay_p(u):
                wait(("dq", u), wrow(u, fq, 0, rows))
                block = wrow(u, fq, g_off, hrows)
                send(("r", u), block, block, to_p, 0)

            def ready(u):
                if u == 0:
                    w_load.wait()
                wait(("r", u), wts.at[u, 0 : 2 * hrows])

            def out_rows(off):
                return outw_hbm.at[pl.ds(al(off, 128), hrows)]

            tok_z(0)
            tok_z(1)
            send(("op", 0), out_rows(f_off), orow(fs, f_off, hrows), to_p, 2)
            for u in range(3):
                direct(u, "q")
                direct(u, "p")
            tok_load.wait()
            gain_load.wait()
            norm(0, 0, 2)
            relay_p(0)
            relay_p(1)
            block = orow(fp, f_off, hrows)
            wait(("op", 0), block)
            send(("orq",), block, block, to_q, 2)
            relay_p(2)
            send(("op", 1), out_rows(g_off), orow(fs, g_off, hrows), to_p, 2)
            relay_q(0)
            tok_f(0)
            relay_q(1)
            tok_w(0)
            norm(1, 0, 1)
            relay_q(2)
            send(("oq", 0), out_rows(g_off), orow(fs, g_off, hrows), to_q, 2)
            send(("oq", 1), out_rows(f_off), orow(fs, f_off, hrows), to_q, 2)
            block = orow(fd, f_off, hrows)
            wait(("orq",), block)
            send(("oz", 0), block, block, to_z, 2)
            for u in range(2):
                ready(u)
                project([u], [0, 1, 2])
            tok_f(1)
            ready(2)
            project([2], [2])
            taps_load.wait()
            tok_w(1)
            norm(1, 1, 1)
            project([0, 1, 2], [3])
            partner_gate(0, None)
            project([2], [0, 1])
            own_gate(0, ("ga",))
            wait(("op", 1), orow(fp, g_off, hrows))
            block = orow(fp, c_off, qrows)
            send(("oz", 1), block, block, to_z, 2)
            block = orow(fq, g_off, hrows)
            wait(("oq", 0), block)
            send(("orp",), block, block, to_p, 2)
            block = orow(fq, c_off, qrows)
            send(("oz", 1), block, block, to_z, 2)
            take(0, None, ("ga",))
            wait(("oq", 1), orow(fq, f_off, hrows))
            ow_load.wait()
            take_other(("ga",), None, 2)
            take(1, None, ("gb",))
            wait(("orp",), orow(fd, g_off, hrows))
            mix(hseq, 0, 2, [(0, 2 * part), (cols, 2 * part)], True, False)
            take_other(("gb",), None, 1)
            mix(hseq, 0, 2, [(2 * part, part), (cols + 2 * part, part)], False, False)
            for h in range(2):
                take(2, h, ("gc", h))
                take_other(("gc", h), h, 1)
                mix(hseq, h, 1, [(3 * part, part), (cols + 3 * part, part)], False, True)
            wait_sent(0, wts.at[0:units, 0 : 6 * hrows])
            wait_sent(1, tok.at[0])
            wait_sent(2, outw)
            wait_sent(3, gat.at[:, 0 : 5 * part])

    @pl.when(inner_chip == 1)
    def _():
        program(True)

    @pl.when(inner_chip == 0)
    def _():
        program(False)

    assert len(cross) <= CROSS


def paired(tokens, norm_gain, outer_weight, inner_weight, value_weight, conv_taps, out_weight):
    _, seq, width = tokens.shape
    rows, cols = outer_weight.shape
    part = cols // PARTS
    anyspace = pl.BlockSpec(memory_space=pltpu.HBM)
    vmem = pl.BlockSpec(memory_space=pltpu.VMEM)
    out = pl.pallas_call(
        kernel,
        out_shape=pltpu.VMEM((seq, cols), BF16),
        in_specs=[anyspace] * 7,
        out_specs=vmem,
        scratch_shapes=[
            pltpu.VMEM((1, width), F32),
            pltpu.VMEM(conv_taps.shape, F32),
            pltpu.VMEM((2, seq, width), BF16),
            pltpu.VMEM((2 * seq, width), BF16),
            pltpu.VMEM((3 * (PARTS - 1), width, part), BF16),
            pltpu.VMEM((width, cols), BF16),
            pltpu.VMEM((3, PARTS - 1, 2, seq + PAD, part), BF16),
            pltpu.VMEM((seq, width), BF16),
            pltpu.VMEM((PARTS - 1, seq, part), BF16),
            pltpu.VMEM((seq, cols), F32),
            pltpu.SemaphoreType.DMA((4,)),
            pltpu.SemaphoreType.DMA((COPIES,)),
            pltpu.SemaphoreType.DMA((5,)),
        ],
        compiler_params=pltpu.CompilerParams(
            collective_id=0, has_side_effects=True, vmem_limit_bytes=58 * 1024 * 1024
        ),
        name="mixer",
    )(
        tokens.reshape(seq, width), norm_gain.reshape(1, width), outer_weight, inner_weight,
        value_weight, conv_taps, out_weight,
    )
    return out.reshape(1, seq, cols)


def solution(mesh):
    shape = dict(mesh.shape)

    def local(tokens, *rest):
        rows, cols = rest[1].shape
        fits = (
            shape["fs"] == 4 and shape["tp"] == 2 and shape["rep"] == 4
            and tokens.shape[0] == 1 and tokens.shape[1] % 256 == 0
            and rows % 512 == 0 and cols == 2 * rows and rest[4].shape[0] <= 9
        )
        return (paired if fits else plain)(tokens, *rest)

    in_specs = (
        P(("rep", "fs"), None, None),
        P(),
        P("fs", "tp"),
        P("fs", "tp"),
        P("fs", "tp"),
        P(),
        P("fs", "tp"),
    )
    out_specs = P(("rep", "fs"), None, "tp")
    return jax.shard_map(local, mesh=mesh, in_specs=in_specs, out_specs=out_specs, check_vma=False)
```

```python
import jax
import jax.numpy as jnp
from jax import lax
from jax.experimental import pallas as pl
from jax.experimental.pallas import tpu as pltpu
from jax.sharding import PartitionSpec as P

MESH = pl.DeviceIdType.MESH
F32 = jnp.float32
BF16 = jnp.bfloat16


def plain(tokens, norm_gain, outer_weight, inner_weight, value_weight, conv_taps, out_weight):
    batch, seq_len, width = tokens.shape
    xf = tokens.astype(F32)
    scale = lax.rsqrt(jnp.mean(xf * xf, axis=-1, keepdims=True) + 1e-06)
    normed = (xf * scale * norm_gain).astype(BF16).reshape(batch * seq_len, width)
    columns = outer_weight.shape[1]

    def project(weight):
        full = lax.all_gather(weight, "fs", axis=0, tiled=True)
        return jnp.dot(normed, full, preferred_element_type=F32).astype(BF16).astype(F32)

    outer, inner, value = project(outer_weight), project(inner_weight), project(value_weight)
    product = (inner * value).reshape(batch, seq_len, columns)
    offset = lax.axis_index("tp") * columns
    taps = lax.dynamic_slice_in_dim(conv_taps, offset, columns, 1)
    count = conv_taps.shape[0]
    padded = jnp.pad(product, ((0, 0), (count - 1, 0), (0, 0)))
    convolved = jnp.zeros((batch, seq_len, columns), F32)
    for k in range(count):
        convolved = convolved + taps[k] * padded[:, k : k + seq_len, :]
    gated = (outer * convolved.reshape(batch * seq_len, columns)).astype(BF16)
    everything = lax.all_gather(gated, "tp", axis=1, tiled=True)
    full = lax.all_gather(out_weight, "fs", axis=0, tiled=True)
    result = jnp.dot(everything, full, preferred_element_type=F32)
    return result.astype(BF16).reshape(batch, seq_len, columns)


PARTS = 4
PAD = 16
CROSS = 9
COPIES = CROSS + 25


def kernel(
    tok_hbm, gain_hbm, outer_hbm, inner_hbm, value_hbm, taps_hbm, outw_hbm, out_ref,
    gain_ref, taps_ref, tok, nm, wts, outw, proj, gat, mine, osum, send_sems, recv_sems, local_sems,
):
    rep, fs, tp = lax.axis_index("rep"), lax.axis_index("fs"), lax.axis_index("tp")
    seq, width = tok_hbm.shape
    rows, cols = outer_hbm.shape
    part = cols // PARTS
    hseq = seq // 2
    hrows = rows // 2
    crows = rows * 9 // 32
    orest = hrows - crows
    count = taps_ref.shape[0]
    m = rep // 2
    inner_chip = lax.rem(rep, 2) + m - 2 * lax.rem(rep, 2) * m
    fx = fs + 1 - 2 * lax.rem(fs, 2)
    fy = lax.rem(fs + 2, 4)
    fd = 3 - fs
    fp = fy + m * (fx - fy)
    fq = fx + m * (fy - fx)
    to_x, to_y, to_p, to_q = (rep, fx, tp), (rep, fy, tp), (rep, fp, tp), (rep, fq, tp)
    to_z, to_t = (rep + 1 - 2 * lax.rem(rep, 2), fs, tp), (rep, fs, 1 - tp)
    to_m = (3 - rep, fs, tp)
    cross = {}

    barrier = pltpu.get_barrier_semaphore()
    for peer in (to_x, to_y, to_z, to_t):
        pl.semaphore_signal(barrier, inc=1, device_id=peer, device_id_type=MESH)

    hbm = (inner_hbm, value_hbm, outer_hbm)
    tok_load = pltpu.make_async_copy(tok_hbm, tok.at[0], local_sems.at[0])
    gain_load = pltpu.make_async_copy(gain_hbm, gain_ref, local_sems.at[1])
    taps_load = pltpu.make_async_copy(taps_hbm, taps_ref, local_sems.at[2])
    gain_load.start()
    taps_load.start()
    tok_load.start()

    def al(x, n):
        return pl.multiple_of(x, n)

    tile = 128

    def norm(s, h, halves):
        @pl.loop(0, halves * hseq // tile)
        def _(b):
            r = al(h * hseq + b * tile, tile)
            xf = tok[s, pl.ds(r, tile), :].astype(F32)
            scale = lax.rsqrt(jnp.mean(xf * xf, axis=-1, keepdims=True) + 1e-06)
            nm[pl.ds(al(s * seq + r, tile), tile), :] = (xf * scale * gain_ref[...]).astype(BF16)

    zeros = jnp.zeros((PAD, part), BF16)
    for c in range(PARTS - 1):
        for w in range(2):
            for s in range(2):
                proj[w, c, s, 0:PAD, :] = zeros

    def project(units, blocks):
        b0, nb = blocks[0], len(blocks)
        u0, nu = units[0], len(units)

        @pl.loop(0, nu * nb)
        def _(i):
            u = u0 + i // nb
            b = b0 + lax.rem(i, nb)
            s, h = b // 2, lax.rem(b, 2)
            d = jnp.dot(nm[pl.ds(al(b * hseq, 128), hseq), :], wts[u], preferred_element_type=F32)
            proj[lax.rem(u, 3), u // 3, s, pl.ds(al(PAD + h * hseq, PAD), hseq), :] = d.astype(BF16)

    def gate(c, first, s, h, halves, store):
        tcols = pl.ds(al(tp * cols + first + c * part, 128), part)

        @pl.loop(0, halves * hseq // tile)
        def _(b):
            r = al(h * hseq + b * tile, tile)
            inner = proj[0, c, s, pl.ds(r, tile + PAD), :].astype(F32)
            value = proj[1, c, s, pl.ds(r, tile + PAD), :].astype(F32)
            outer = proj[2, c, s, pl.ds(al(r + PAD, PAD), tile), :].astype(F32)
            window = inner * value
            conv = jnp.zeros((tile, part), F32)
            for k in range(count):
                lo = PAD - (count - 1) + k
                conv = conv + taps_ref[k : k + 1, tcols] * window[lo : lo + tile, :]
            store(pl.ds(r, tile), (outer * conv).astype(BF16))

    def mix(h, terms, first, last):
        r = slice(0, seq) if h is None else slice(h * hseq, (h + 1) * hseq)

        for b in range(cols // part):
            at = slice(b * part, (b + 1) * part)
            total = None
            for k, n in terms:
                d = jnp.dot(gat[r, pl.ds(k, n)], outw[pl.ds(k, n), at], preferred_element_type=F32)
                total = d if total is None else total + d
            if not first:
                total = total + osum[r, at]
            if last:
                out_ref[r, at] = total.astype(BF16)
            else:
                osum[r, at] = total

    def program(inside):
        local = {}

        def index(key):
            if key[0] in ("tz", "gz", "oz"):
                return cross.setdefault(key, len(cross))
            return CROSS + local.setdefault(key, len(local))

        def send(key, src, dst, device, group):
            k = index(key)
            pltpu.make_async_remote_copy(
                src_ref=src, dst_ref=dst, send_sem=send_sems.at[group], recv_sem=recv_sems.at[k],
                device_id=device, device_id_type=MESH,
            ).start()

        def wait(key, dst):
            k = index(key)
            pltpu.make_async_remote_copy(
                src_ref=dst, dst_ref=dst, send_sem=send_sems.at[0], recv_sem=recv_sems.at[k],
                device_id=to_t, device_id_type=MESH,
            ).wait_recv()

        def wait_sent(group, src):
            pltpu.make_async_remote_copy(
                src_ref=src, dst_ref=src, send_sem=send_sems.at[group], recv_sem=recv_sems.at[0],
                device_id=to_t, device_id_type=MESH,
            ).wait_send()

        chunks = PARTS - 1 if inside else 1
        first = part if inside else 0
        other_chunks = PARTS - chunks
        other_first = 0 if inside else part
        units = 3 * chunks
        for u in range(units):
            c, w = u // 3, u % 3
            pltpu.make_async_copy(
                hbm[w].at[:, pl.ds(first + c * part, part)],
                wts.at[u, pl.ds(al(fs * rows, rows), rows)], local_sems.at[3],
            ).start()
        w_load = pltpu.make_async_copy(
            wts.at[0:units, 0:rows], wts.at[0:units, 0:rows], local_sems.at[3])
        ow_load = pltpu.make_async_copy(
            outw_hbm, outw.at[pl.ds(al(fs * rows, rows), rows)], local_sems.at[4])
        ow_load.start()

        def wrow(u, f, off, n):
            return wts.at[u, pl.ds(al(f * rows + off, 128), n)]

        def orow(f, off, n):
            return outw.at[pl.ds(al(f * rows + off, 16), n)]

        def trow(h, t):
            return pl.ds(al(h * hseq + t * (hseq // 2), 64), hseq // 2)

        def tok_z(h):
            send(("tz", h), tok_hbm.at[trow(h, tp)], tok.at[1, trow(h, tp)], to_z, 1)

        def tok_f(h):
            here = tok.at[1, trow(h, tp)]
            wait(("tz", h), here)
            send(("tt", h), here, here, to_t, 1)

        def tok_w(h):
            wait(("tt", h), tok.at[1, trow(h, 1 - tp)])

        def gcols(t, base, c):
            return pl.ds(al(t * cols + base + c * part, 128), part)

        def grow(h):
            return pl.ds(0, seq) if h is None else pl.ds(h * hseq, hseq)

        def z_key(c, h, from_inside):
            return ("gz", c, h if from_inside and c == PARTS - 2 else None, from_inside)

        def own_gate(c, key):
            def store(r, x):
                gat[r, gcols(tp, first, c)] = x
            gate(c, first, 0, 0, 2, store)
            here = gat.at[:, gcols(tp, first, c)]
            send(key, here, here, to_t, 3)

        def partner_gate(c, h):
            def store(r, x):
                mine[c, r, :] = x
            gate(c, first, 1, h or 0, 2 if h is None else 1, store)
            send(z_key(c, h, inside), mine.at[c, grow(h)], gat.at[grow(h), gcols(tp, first, c)], to_z, 3)

        def take(c, h, key):
            here = gat.at[grow(h), gcols(tp, other_first, c)]
            wait(z_key(c, h, not inside), here)
            send(key, here, here, to_t, 3)

        def take_other(key, h, parts):
            wait(key, gat.at[grow(h), pl.ds(0, parts * part)])

        f_off, g_off = m * hrows, (1 - m) * hrows
        c_off, o_off = g_off + (1 - m) * orest, g_off + m * crows

        if inside:
            pl.semaphore_signal(barrier, inc=1, device_id=to_m, device_id_type=MESH)
            pl.semaphore_wait(barrier, 5)
            hx, hy = m * hrows, (1 - m) * hrows

            def direct(u):
                c, w = u // 3, u % 3
                at = pl.ds(first + c * part, part)
                send(("d", u), hbm[w].at[pl.ds(al(hx, 128), hrows), at], wrow(u, fs, hx, hrows), to_x, 0)
                send(("d", u), hbm[w].at[pl.ds(al(hy, 128), hrows), at], wrow(u, fs, hy, hrows), to_y, 0)

            def relay(u):
                wait(("d", u), wts.at[u, 0 : 2 * hrows])
                bx, by = wrow(u, fx, hx, hrows), wrow(u, fy, hy, hrows)
                send(("r", u), bx, bx, to_m, 0)
                send(("r", u), by, by, to_x, 0)
                send(("r", u), bx, bx, to_y, 0)
                send(("r", u), by, by, to_m, 0)

            def ready(u):
                if u == 0:
                    w_load.wait()
                wait(("r", u), wts.at[u, 0 : 4 * hrows])

            tok_z(0)
            tok_z(1)
            for u in range(3):
                direct(u)
            tok_load.wait()
            gain_load.wait()
            norm(0, 0, 2)
            relay(0)
            direct(3)
            relay(1)
            direct(4)
            relay(2)
            direct(5)
            ready(0)
            project([0], [0, 1])
            relay(3)
            direct(6)
            ready(1)
            project([1], [0, 1])
            tok_f(0)
            relay(4)
            direct(7)
            tok_w(0)
            norm(1, 0, 1)
            ready(2)
            project([2], [0, 1])
            project([0, 1, 2], [2])
            taps_load.wait()
            partner_gate(0, 0)
            own_gate(0, ("ga",))
            relay(5)
            direct(8)
            ready(3)
            project([3], [0, 1, 2])
            relay(6)
            ready(4)
            project([4], [0, 1, 2])
            tok_f(1)
            relay(7)
            tok_w(1)
            norm(1, 1, 1)
            project([0, 1, 2], [3])
            partner_gate(0, 1)
            relay(8)
            for b, (off, n) in enumerate(((f_off, hrows), (o_off, orest))):
                src = outw_hbm.at[pl.ds(al(off, 16), n)]
                send(("o", b), src, orow(fs, off, n), to_x, 2)
                send(("o", b), src, orow(fs, off, n), to_y, 2)
            ready(5)
            project([5], [0, 1, 2])
            partner_gate(1, 0)
            project([3, 4, 5], [3])
            partner_gate(1, 1)
            own_gate(1, ("ga",))
            wait(("oz", 0), orow(fd, f_off, hrows))

            def swap():
                block = orow(fd, f_off, hrows)
                send(("om",), block, block, to_m, 2)

            pl.when(tp == 0)(swap)
            ready(6)
            project([6], [0, 1, 2, 3])
            ready(7)
            project([7], [0, 1, 2, 3])
            ready(8)
            project([8], [2])
            partner_gate(2, 0)
            project([8], [3])
            partner_gate(2, 1)
            pl.when(tp == 1)(swap)
            project([8], [0, 1])
            own_gate(2, ("ga",))
            take(0, None, ("ga",))
            ow_load.wait()
            take_other(("ga",), None, PARTS)
            def krow(f, off):
                return al(f * rows + off, 128), hrows

            mix(None, [(al(fs * rows, rows), rows), krow(fd, f_off)], True, False)
            wait(("o", 0), outw.at[0 : 2 * hrows])
            mix(None, [krow(fx, f_off), krow(fy, f_off)], False, False)
            wait(("om",), orow(fd, g_off, hrows))
            mix(None, [krow(fd, g_off)], False, False)
            wait(("oz", 1), outw.at[0 : 2 * crows])
            wait(("o", 1), outw.at[0 : 2 * orest])
            mix(None, [krow(fx, g_off), krow(fy, g_off)], False, True)
            wait_sent(0, wts.at[:, 0 : 6 * hrows])
            wait_sent(1, tok.at[0])
            wait_sent(2, outw.at[0 : 3 * hrows + 2 * orest])
            wait_sent(3, gat.at[:, 0 : 7 * part])
        else:
            pl.semaphore_wait(barrier, 4)

            def direct(u, which):
                c, w = u // 3, u % 3
                src = hbm[w].at[:, pl.ds(first + c * part, part)]
                send(("d" + which, u), src, wrow(u, fs, 0, rows), to_p if which == "p" else to_q, 0)

            def relay_q(u):
                wait(("dp", u), wrow(u, fp, 0, rows))
                block = wrow(u, fp, f_off, hrows)
                send(("r", u), block, block, to_q, 0)

            def relay_p(u):
                wait(("dq", u), wrow(u, fq, 0, rows))
                block = wrow(u, fq, g_off, hrows)
                send(("r", u), block, block, to_p, 0)

            def ready(u):
                if u == 0:
                    w_load.wait()
                wait(("r", u), wts.at[u, 0 : 2 * hrows])

            def out_rows(off):
                return outw_hbm.at[pl.ds(al(off, 16), hrows)]

            tok_z(0)
            tok_z(1)
            send(("op", 0), out_rows(f_off), orow(fs, f_off, hrows), to_p, 2)
            for u in range(3):
                direct(u, "q")
                direct(u, "p")
            tok_load.wait()
            gain_load.wait()
            norm(0, 0, 2)
            relay_p(0)
            relay_p(1)
            block = orow(fp, f_off, hrows)
            wait(("op", 0), block)
            send(("orq",), block, block, to_q, 2)
            relay_p(2)
            send(("op", 1), out_rows(g_off), orow(fs, g_off, hrows), to_p, 2)
            relay_q(0)
            tok_f(0)
            relay_q(1)
            tok_w(0)
            norm(1, 0, 1)
            relay_q(2)
            send(("oq", 0), out_rows(g_off), orow(fs, g_off, hrows), to_q, 2)
            send(("oq", 1), out_rows(f_off), orow(fs, f_off, hrows), to_q, 2)
            block = orow(fd, f_off, hrows)
            wait(("orq",), block)
            send(("oz", 0), block, block, to_z, 2)
            for u in range(2):
                ready(u)
                project([u], [0, 1, 2])
            tok_f(1)
            ready(2)
            project([2], [2])
            taps_load.wait()
            tok_w(1)
            norm(1, 1, 1)
            project([0, 1, 2], [3])
            partner_gate(0, None)
            project([2], [0, 1])
            own_gate(0, ("ga",))
            wait(("op", 1), orow(fp, g_off, hrows))
            block = orow(fp, c_off, crows)
            send(("oz", 1), block, block, to_z, 4)
            block = orow(fq, g_off, hrows)
            wait(("oq", 0), block)
            send(("orp",), block, block, to_p, 2)
            block = orow(fq, c_off, crows)
            send(("oz", 1), block, block, to_z, 4)
            take(0, None, ("ga",))
            wait(("oq", 1), orow(fq, f_off, hrows))
            ow_load.wait()
            take_other(("ga",), None, 2)
            take(1, None, ("gb",))
            wait(("orp",), orow(fd, g_off, hrows))
            mix(None, [(0, 2 * part), (cols, 2 * part)], True, False)
            take_other(("gb",), None, 1)
            mix(None, [(2 * part, part), (cols + 2 * part, part)], False, False)
            for h in range(2):
                take(2, h, ("gc", h))
            for h in range(2):
                take_other(("gc", h), h, 1)
                mix(h, [(3 * part, part), (cols + 3 * part, part)], False, True)
            wait_sent(0, wts.at[0:units, 0 : 6 * hrows])
            wait_sent(1, tok.at[0])
            wait_sent(2, outw.at[0 : 7 * hrows])
            wait_sent(3, gat.at[:, 0 : 5 * part])
            wait_sent(4, outw.at[0 : 2 * crows])

    @pl.when(inner_chip == 1)
    def _():
        program(True)

    @pl.when(inner_chip == 0)
    def _():
        program(False)

    assert len(cross) <= CROSS


def paired(tokens, norm_gain, outer_weight, inner_weight, value_weight, conv_taps, out_weight):
    _, seq, width = tokens.shape
    rows, cols = outer_weight.shape
    part = cols // PARTS
    anyspace = pl.BlockSpec(memory_space=pltpu.HBM)
    vmem = pl.BlockSpec(memory_space=pltpu.VMEM)
    out = pl.pallas_call(
        kernel,
        out_shape=pltpu.VMEM((seq, cols), BF16),
        in_specs=[anyspace] * 7,
        out_specs=vmem,
        scratch_shapes=[
            pltpu.VMEM((1, width), F32),
            pltpu.VMEM(conv_taps.shape, F32),
            pltpu.VMEM((2, seq, width), BF16),
            pltpu.VMEM((2 * seq, width), BF16),
            pltpu.VMEM((3 * (PARTS - 1), width, part), BF16),
            pltpu.VMEM((width, cols), BF16),
            pltpu.VMEM((3, PARTS - 1, 2, seq + PAD, part), BF16),
            pltpu.VMEM((seq, width), BF16),
            pltpu.VMEM((PARTS - 1, seq, part), BF16),
            pltpu.VMEM((seq, cols), F32),
            pltpu.SemaphoreType.DMA((5,)),
            pltpu.SemaphoreType.DMA((COPIES,)),
            pltpu.SemaphoreType.DMA((5,)),
        ],
        compiler_params=pltpu.CompilerParams(
            collective_id=0, has_side_effects=True, vmem_limit_bytes=58 * 1024 * 1024
        ),
        name="mixer",
    )(
        tokens.reshape(seq, width), norm_gain.reshape(1, width), outer_weight, inner_weight,
        value_weight, conv_taps, out_weight,
    )
    return out.reshape(1, seq, cols)


def solution(mesh):
    shape = dict(mesh.shape)

    def local(tokens, *rest):
        rows, cols = rest[1].shape
        fits = (
            shape["fs"] == 4 and shape["tp"] == 2 and shape["rep"] == 4
            and tokens.shape[0] == 1 and tokens.shape[1] % 256 == 0
            and rows % 512 == 0 and cols == 2 * rows and rest[4].shape[0] <= 9
        )
        return (paired if fits else plain)(tokens, *rest)

    in_specs = (
        P(("rep", "fs"), None, None),
        P(),
        P("fs", "tp"),
        P("fs", "tp"),
        P("fs", "tp"),
        P(),
        P("fs", "tp"),
    )
    out_specs = P(("rep", "fs"), None, "tp")
    return jax.shard_map(local, mesh=mesh, in_specs=in_specs, out_specs=out_specs, check_vma=False)
```

```python
import jax
import jax.numpy as jnp
from jax import lax
from jax.experimental import pallas as pl
from jax.experimental.pallas import tpu as pltpu
from jax.sharding import PartitionSpec as P

MESH = pl.DeviceIdType.MESH
F32 = jnp.float32
BF16 = jnp.bfloat16


def plain(tokens, norm_gain, outer_weight, inner_weight, value_weight, conv_taps, out_weight):
    batch, seq_len, width = tokens.shape
    xf = tokens.astype(F32)
    scale = lax.rsqrt(jnp.mean(xf * xf, axis=-1, keepdims=True) + 1e-06)
    normed = (xf * scale * norm_gain).astype(BF16).reshape(batch * seq_len, width)
    columns = outer_weight.shape[1]

    def project(weight):
        full = lax.all_gather(weight, "fs", axis=0, tiled=True)
        return jnp.dot(normed, full, preferred_element_type=F32).astype(BF16).astype(F32)

    outer, inner, value = project(outer_weight), project(inner_weight), project(value_weight)
    product = (inner * value).reshape(batch, seq_len, columns)
    offset = lax.axis_index("tp") * columns
    taps = lax.dynamic_slice_in_dim(conv_taps, offset, columns, 1)
    count = conv_taps.shape[0]
    padded = jnp.pad(product, ((0, 0), (count - 1, 0), (0, 0)))
    convolved = jnp.zeros((batch, seq_len, columns), F32)
    for k in range(count):
        convolved = convolved + taps[k] * padded[:, k : k + seq_len, :]
    gated = (outer * convolved.reshape(batch * seq_len, columns)).astype(BF16)
    everything = lax.all_gather(gated, "tp", axis=1, tiled=True)
    full = lax.all_gather(out_weight, "fs", axis=0, tiled=True)
    result = jnp.dot(everything, full, preferred_element_type=F32)
    return result.astype(BF16).reshape(batch, seq_len, columns)


PARTS = 4
PAD = 16
CROSS = 10
COPIES = CROSS + 31


def kernel(
    tok_hbm, gain_hbm, outer_hbm, inner_hbm, value_hbm, taps_hbm, outw_hbm, out_ref,
    gain_ref, taps_ref, tok, nm, wts, outw, proj, gat, mine, osum, send_sems, recv_sems, local_sems,
):
    rep, fs, tp = lax.axis_index("rep"), lax.axis_index("fs"), lax.axis_index("tp")
    seq, width = tok_hbm.shape
    rows, cols = outer_hbm.shape
    part = cols // PARTS
    hseq = seq // 2
    hrows = rows // 2
    hpart = part // 2
    crows = rows * 6 // 32
    zrows = rows // 8
    orest = hrows - crows
    count = taps_ref.shape[0]
    m = rep // 2
    inner_chip = lax.rem(rep, 2) + m - 2 * lax.rem(rep, 2) * m
    fx = fs + 1 - 2 * lax.rem(fs, 2)
    fy = lax.rem(fs + 2, 4)
    fd = 3 - fs
    fp = fy + m * (fx - fy)
    fq = fx + m * (fy - fx)
    to_x, to_y, to_p, to_q = (rep, fx, tp), (rep, fy, tp), (rep, fp, tp), (rep, fq, tp)
    to_z, to_t = (rep + 1 - 2 * lax.rem(rep, 2), fs, tp), (rep, fs, 1 - tp)
    to_m = (3 - rep, fs, tp)
    cross = {}

    barrier = pltpu.get_barrier_semaphore()
    for peer in (to_x, to_y, to_z, to_t):
        pl.semaphore_signal(barrier, inc=1, device_id=peer, device_id_type=MESH)

    hbm = (inner_hbm, value_hbm, outer_hbm)
    tok_load = pltpu.make_async_copy(tok_hbm, tok.at[0], local_sems.at[0])
    gain_load = pltpu.make_async_copy(gain_hbm, gain_ref, local_sems.at[1])
    taps_load = pltpu.make_async_copy(taps_hbm, taps_ref, local_sems.at[2])
    gain_load.start()
    taps_load.start()
    tok_load.start()

    def al(x, n):
        return pl.multiple_of(x, n)

    tile = 128

    def norm(s, h, halves):
        @pl.loop(0, halves * hseq // tile)
        def _(b):
            r = al(h * hseq + b * tile, tile)
            xf = tok[s, pl.ds(r, tile), :].astype(F32)
            scale = lax.rsqrt(jnp.mean(xf * xf, axis=-1, keepdims=True) + 1e-06)
            nm[pl.ds(al(s * seq + r, tile), tile), :] = (xf * scale * gain_ref[...]).astype(BF16)

    zeros = jnp.zeros((PAD, part), BF16)
    for c in range(PARTS - 1):
        for w in range(2):
            for s in range(2):
                proj[w, c, s, 0:PAD, :] = zeros

    def project(units, blocks):
        b0, nb = blocks[0], len(blocks)
        u0, nu = units[0], len(units)

        @pl.loop(0, nu * nb)
        def _(i):
            u = u0 + i // nb
            b = b0 + lax.rem(i, nb)
            s, h = b // 2, lax.rem(b, 2)
            d = jnp.dot(nm[pl.ds(al(b * hseq, 128), hseq), :], wts[u], preferred_element_type=F32)
            proj[lax.rem(u, 3), u // 3, s, pl.ds(al(PAD + h * hseq, PAD), hseq), :] = d.astype(BF16)

    def gate(c, first, s, h, halves, store):
        tcols = pl.ds(al(tp * cols + first + c * part, 128), part)

        @pl.loop(0, halves * hseq // tile)
        def _(b):
            r = al(h * hseq + b * tile, tile)
            inner = proj[0, c, s, pl.ds(r, tile + PAD), :].astype(F32)
            value = proj[1, c, s, pl.ds(r, tile + PAD), :].astype(F32)
            outer = proj[2, c, s, pl.ds(al(r + PAD, PAD), tile), :].astype(F32)
            window = inner * value
            conv = jnp.zeros((tile, part), F32)
            for k in range(count):
                lo = PAD - (count - 1) + k
                conv = conv + taps_ref[k : k + 1, tcols] * window[lo : lo + tile, :]
            store(pl.ds(r, tile), (outer * conv).astype(BF16))

    def mix(h, terms, first, last):
        r = slice(0, seq) if h is None else slice(h * hseq, (h + 1) * hseq)

        for b in range(cols // part):
            at = slice(b * part, (b + 1) * part)
            total = None
            for k, n in terms:
                d = jnp.dot(gat[r, pl.ds(k, n)], outw[pl.ds(k, n), at], preferred_element_type=F32)
                total = d if total is None else total + d
            if not first:
                total = total + osum[r, at]
            if last:
                out_ref[r, at] = total.astype(BF16)
            else:
                osum[r, at] = total

    def program(inside):
        local = {}

        def index(key):
            if key[0] in ("tz", "gz", "ge", "oz"):
                return cross.setdefault(key, len(cross))
            return CROSS + local.setdefault(key, len(local))

        def send(key, src, dst, device, group):
            k = index(key)
            pltpu.make_async_remote_copy(
                src_ref=src, dst_ref=dst, send_sem=send_sems.at[group], recv_sem=recv_sems.at[k],
                device_id=device, device_id_type=MESH,
            ).start()

        def wait(key, dst):
            k = index(key)
            pltpu.make_async_remote_copy(
                src_ref=dst, dst_ref=dst, send_sem=send_sems.at[0], recv_sem=recv_sems.at[k],
                device_id=to_t, device_id_type=MESH,
            ).wait_recv()

        def wait_sent(group, src):
            pltpu.make_async_remote_copy(
                src_ref=src, dst_ref=src, send_sem=send_sems.at[group], recv_sem=recv_sems.at[0],
                device_id=to_t, device_id_type=MESH,
            ).wait_send()

        chunks = PARTS - 1 if inside else 2
        first = part if inside else 0
        units = 3 * chunks

        def split(c):
            return c == (0 if inside else 1)

        def widths(c, act):
            if not split(c):
                act(0, part)
                return
            pl.when(tp == 0)(lambda: act(hpart if inside else 0, hpart))
            if inside:
                pl.when(tp == 1)(lambda: act(0, part))

        for u in range(units):
            c, w = u // 3, u % 3
            pltpu.make_async_copy(
                hbm[w].at[:, pl.ds(first + c * part, part)],
                wts.at[u, pl.ds(al(fs * rows, rows), rows)], local_sems.at[3],
            ).start()
        w_load = pltpu.make_async_copy(
            wts.at[0:units, 0:rows], wts.at[0:units, 0:rows], local_sems.at[3])
        ow_load = pltpu.make_async_copy(
            outw_hbm, outw.at[pl.ds(al(fs * rows, rows), rows)], local_sems.at[4])
        ow_load.start()

        def wrow(u, f, off, n, lo, wd):
            return wts.at[u, pl.ds(al(f * rows + off, 128), n), pl.ds(lo, wd)]

        def orow(f, off, n):
            return outw.at[pl.ds(al(f * rows + off, 16), n)]

        def trow(h, t):
            return pl.ds(al(h * hseq + t * (hseq // 2), 64), hseq // 2)

        def tok_z(h):
            send(("tz", h), tok_hbm.at[trow(h, tp)], tok.at[1, trow(h, tp)], to_z, 1)

        def tok_f(h):
            here = tok.at[1, trow(h, tp)]
            wait(("tz", h), here)
            send(("tt", h), here, here, to_t, 1)

        def tok_w(h):
            wait(("tt", h), tok.at[1, trow(h, 1 - tp)])

        def gcols(c, lo, wd):
            return pl.ds(al(tp * cols + first + c * part + lo, 128), wd)

        def grow(h):
            return pl.ds(0, seq) if h is None else pl.ds(h * hseq, hseq)

        def own_gate(c, key):
            def store(r, x):
                def act(lo, wd):
                    gat[r, gcols(c, lo, wd)] = x[:, lo : lo + wd]
                widths(c, act)

            def out(lo, wd):
                here = gat.at[:, gcols(c, lo, wd)]
                send(key, here, here, to_t, 3)

            def run():
                gate(c, first, 0, 0, 2, store)
                widths(c, out)

            if split(c) and not inside:
                pl.when(tp == 0)(run)
            else:
                run()

        def partner_gate(c, h):
            key = ("gz", c, h if c == PARTS - 2 else None) if inside else ("ge",)

            def store(r, x):
                mine[c, r, :] = x

            def out(lo, wd):
                src = mine.at[c, grow(h), pl.ds(lo, wd)]
                send(key, src, gat.at[grow(h), gcols(c, lo, wd)], to_z, 3)

            def run():
                gate(c, first, 1, h or 0, 2 if h is None else 1, store)
                widths(c, out)

            if split(c) and not inside:
                pl.when(tp == 0)(run)
            else:
                run()

        def forward(key, h, at, wd, new):
            here = gat.at[grow(h), pl.ds(al(tp * cols + at, 128), wd)]
            wait(key, here)
            send(new, here, here, to_t, 3)

        def take_other(key, h, parts):
            wait(key, gat.at[grow(h), pl.ds(0, parts * part)])

        f_off, g_off = m * hrows, (1 - m) * hrows
        c_off, o_off = g_off + (1 - m) * orest, g_off + m * crows
        zp_off, zq_off = g_off + m * (hrows - zrows), f_off + (1 - m) * (hrows - zrows)

        def krow(f, off):
            return al(f * rows + off, 128), hrows


        if inside:
            pl.semaphore_signal(barrier, inc=1, device_id=to_m, device_id_type=MESH)
            pl.semaphore_wait(barrier, 5)
            hx, hy = m * hrows, (1 - m) * hrows

            def direct(u):
                c, w = u // 3, u % 3

                def act(lo, wd):
                    at = pl.ds(first + c * part + lo, wd)
                    for off, to in ((hx, to_x), (hy, to_y)):
                        src = hbm[w].at[pl.ds(al(off, 128), hrows), at]
                        send(("d", u), src, wrow(u, fs, off, hrows, lo, wd), to, 0)
                widths(c, act)

            def relay(u):
                def act(lo, wd):
                    wait(("d", u), wts.at[u, 0 : 2 * hrows, lo : lo + wd])
                    bx, by = wrow(u, fx, hx, hrows, lo, wd), wrow(u, fy, hy, hrows, lo, wd)
                    send(("r", u), bx, bx, to_m, 0)
                    send(("r", u), by, by, to_x, 0)
                    send(("r", u), bx, bx, to_y, 0)
                    send(("r", u), by, by, to_m, 0)
                widths(u // 3, act)

            def ready(u):
                if u == 0:
                    w_load.wait()
                widths(u // 3, lambda lo, wd: wait(("r", u), wts.at[u, 0 : 4 * hrows, lo : lo + wd]))

            def out_rows(key, off, n, to):
                send(key, outw_hbm.at[pl.ds(al(off, 16), n)], orow(fs, off, n), to, 2)

            tok_z(0)
            tok_z(1)
            for u in range(3):
                direct(u)
            tok_load.wait()
            gain_load.wait()
            norm(0, 0, 2)
            relay(0)
            direct(3)
            relay(1)
            direct(4)
            relay(2)
            direct(5)
            ready(0)
            project([0], [0, 1])
            relay(3)
            direct(6)
            out_rows(("oe",), zp_off, zrows, to_p)
            out_rows(("oe",), zq_off, zrows, to_q)
            ready(1)
            project([1], [0, 1])
            tok_f(0)
            relay(4)
            direct(7)
            tok_w(0)
            norm(1, 0, 1)
            ready(2)
            project([2], [0, 1])
            project([0, 1, 2], [2])
            taps_load.wait()
            partner_gate(0, 0)
            own_gate(0, ("ga",))
            relay(5)
            direct(8)
            ready(3)
            project([3], [0, 1, 2])
            relay(6)
            wait(("oe",), outw.at[0 : 2 * zrows])
            for f, off in ((fp, zp_off), (fq, zq_off)):
                block = orow(f, off, zrows)
                send(("oz", 2), block, block, to_z, 2)
            ready(4)
            tok_f(1)
            project([4], [0, 1, 2])
            relay(7)
            tok_w(1)
            norm(1, 1, 1)
            project([0, 1, 2], [3])
            partner_gate(0, 1)
            relay(8)
            out_rows(("o", 0), f_off, hrows, to_p)
            out_rows(("o", 0), f_off + m * zrows, hrows - zrows, to_q)
            out_rows(("o", 1), o_off + (1 - m) * zrows, orest - zrows, to_p)
            out_rows(("o", 1), o_off, orest, to_q)
            ready(5)
            project([5], [0, 1, 2])
            partner_gate(1, 0)
            project([3, 4, 5], [3])
            partner_gate(1, 1)
            own_gate(1, ("ga",))
            wait(("oz", 0), orow(fd, f_off, hrows))

            def swap():
                block = orow(fd, f_off, hrows)
                send(("om",), block, block, to_m, 2)

            pl.when(tp == 0)(swap)
            ready(6)
            project([6], [0, 1, 2, 3])
            ready(7)
            project([7], [0, 1, 2, 3])
            ready(8)
            project([8], [2])
            partner_gate(2, 0)
            project([8], [3])
            partner_gate(2, 1)
            pl.when(tp == 1)(swap)
            project([8], [0, 1])
            own_gate(2, ("ga",))
            pl.when(tp == 0)(lambda: forward(("ge",), None, 0, part + hpart, ("ga",)))
            pl.when(tp == 1)(lambda: forward(("ge",), None, 0, part, ("ga",)))
            ow_load.wait()
            take_other(("ga",), None, PARTS)
            mix(None, [(al(fs * rows, rows), rows), krow(fd, f_off)], True, False)
            wait(("o", 0), outw.at[0 : 2 * hrows - zrows])
            mix(None, [krow(fx, f_off), krow(fy, f_off)], False, False)
            wait(("om",), orow(fd, g_off, hrows))
            mix(None, [krow(fd, g_off)], False, False)
            wait(("oz", 1), outw.at[0 : 2 * crows])
            wait(("o", 1), outw.at[0 : 2 * orest - zrows])
            mix(None, [krow(fx, g_off), krow(fy, g_off)], False, True)
            pl.when(tp == 0)(lambda: wait_sent(0, wts.at[:, 0 : 5 * hrows]))
            pl.when(tp == 1)(lambda: wait_sent(0, wts.at[:, 0 : 6 * hrows]))
            wait_sent(1, tok.at[0])
            wait_sent(2, outw.at[0 : 3 * hrows + 2 * orest + 2 * zrows])
            pl.when(tp == 0)(lambda: wait_sent(3, gat.at[:, 0 : 13 * hpart]))
            pl.when(tp == 1)(lambda: wait_sent(3, gat.at[:, 0 : 14 * hpart]))
        else:
            pl.semaphore_wait(barrier, 4)

            def direct(u, which):
                c, w = u // 3, u % 3
                wd = hpart if split(c) else part
                src = hbm[w].at[:, pl.ds(first + c * part, wd)]
                send(("d" + which, u), src, wrow(u, fs, 0, rows, 0, wd), to_p if which == "p" else to_q, 0)

            def relay_q(u):
                wd = hpart if split(u // 3) else part
                wait(("dp", u), wrow(u, fp, 0, rows, 0, wd))
                block = wrow(u, fp, f_off, hrows, 0, wd)
                send(("r", u), block, block, to_q, 0)

            def relay_p(u):
                wd = hpart if split(u // 3) else part
                wait(("dq", u), wrow(u, fq, 0, rows, 0, wd))
                block = wrow(u, fq, g_off, hrows, 0, wd)
                send(("r", u), block, block, to_p, 0)

            def ready(u):
                if u == 0:
                    w_load.wait()
                wd = hpart if split(u // 3) else part
                wait(("r", u), wts.at[u, 0 : 2 * hrows, 0:wd])

            def out_rows(key, off, n, to):
                send(key, outw_hbm.at[pl.ds(al(off, 16), n)], orow(fs, off, n), to, 2)

            extra = pl.when(tp == 0)

            tok_z(0)
            tok_z(1)
            out_rows(("op", 0), f_off, hrows, to_p)
            for u in range(3):
                direct(u, "q")
                direct(u, "p")

            @extra
            def _():
                for u in range(3, 6):
                    direct(u, "p")

            tok_load.wait()
            gain_load.wait()
            norm(0, 0, 2)
            relay_p(0)
            relay_p(1)
            block = orow(fp, f_off, hrows)
            wait(("op", 0), block)
            send(("orq",), block, block, to_q, 2)

            @extra
            def _():
                for u in range(3, 6):
                    direct(u, "q")


            relay_p(2)
            relay_q(0)
            tok_f(0)
            relay_q(1)
            tok_w(0)
            norm(1, 0, 1)
            relay_q(2)
            block = orow(fd, f_off, hrows)
            wait(("orq",), block)
            send(("oz", 0), block, block, to_z, 2)

            tok_f(1)
            ready(0)
            project([0], [0, 1, 2])

            @extra
            def _():
                for u in range(3, 6):
                    relay_p(u)
                    relay_q(u)

            ready(1)
            project([1], [0, 1, 2])
            out_rows(("op", 1), g_off + (1 - m) * zrows, hrows - zrows, to_p)
            for b in range(2):
                out_rows(("oq", b), g_off + b * hrows // 2, hrows // 2, to_q)
            out_rows(("oq", 2), f_off + m * zrows, hrows - zrows, to_q)
            tok_w(1)
            norm(1, 1, 1)
            ready(2)
            taps_load.wait()
            project([2], [2])
            project([0, 1, 2], [3])
            partner_gate(0, None)

            @extra
            def _():
                for u in range(3, 6):
                    ready(u)
                project([3, 4, 5], [2, 3])
            partner_gate(1, None)
            def pass_on(b):
                block = orow(fq, g_off + b * hrows // 2, hrows // 2)
                wait(("oq", b), block)
                send(("orp",), block, block, to_p, 2)

            project([2], [0, 1])
            own_gate(0, ("ga",))
            pass_on(0)
            extra(lambda: project([3, 4], [0, 1]))
            wait(("op", 1), orow(fp, g_off, hrows - zrows))
            block = orow(fp, c_off, crows)
            send(("oz", 1), block, block, to_z, 4)
            extra(lambda: project([5], [0, 1]))
            own_gate(1, ("ga",))
            pl.when(tp == 0)(lambda: forward(("gz", 0, None), None, part + hpart, hpart, ("ga",)))
            pl.when(tp == 1)(lambda: forward(("gz", 0, None), None, part, part, ("ga",)))
            pass_on(1)
            block = orow(fq, c_off, crows)
            send(("oz", 1), block, block, to_z, 4)
            forward(("gz", 1, None), None, 2 * part, part, ("gb",))
            ow_load.wait()
            take_other(("ga",), None, 2)
            take_other(("gb",), None, 1)
            wait(("oz", 2), outw.at[0 : 2 * zrows])
            odd = lax.rem(fs, 2)
            mix(None, [krow(fs, 0), krow(fp, 0), krow(fd + m * (fq - fd), 0),
                       krow(fs + odd * (fx - fs), hrows)], True, False)
            for h in range(2):
                forward(("gz", 2, h), h, 3 * part, part, ("gc", h))
            wait(("oq", 2), orow(fq, f_off, hrows - zrows))
            for h in range(2):
                take_other(("gc", h), h, 1)
                mix(h, [krow(fq, f_off), krow(fp + m * (fd - fp), hrows),
                        krow(fx + odd * (fs - fx), hrows)], False, False)
            wait(("orp",), orow(fd, g_off, hrows))
            mix(None, [krow(fd, g_off)], False, True)
            pl.when(tp == 0)(lambda: wait_sent(0, wts.at[0:6, 0 : 9 * hrows // 2]))
            pl.when(tp == 1)(lambda: wait_sent(0, wts.at[0:3, 0 : 6 * hrows]))
            wait_sent(1, tok.at[0])
            wait_sent(2, outw.at[0 : 7 * hrows - 2 * zrows])
            pl.when(tp == 0)(lambda: wait_sent(3, gat.at[:, 0 : 11 * hpart]))
            pl.when(tp == 1)(lambda: wait_sent(3, gat.at[:, 0 : 10 * hpart]))
            wait_sent(4, outw.at[0 : 2 * crows])

    @pl.when(inner_chip == 1)
    def _():
        program(True)

    @pl.when(inner_chip == 0)
    def _():
        program(False)

    assert len(cross) <= CROSS


def paired(tokens, norm_gain, outer_weight, inner_weight, value_weight, conv_taps, out_weight):
    _, seq, width = tokens.shape
    rows, cols = outer_weight.shape
    part = cols // PARTS
    anyspace = pl.BlockSpec(memory_space=pltpu.HBM)
    vmem = pl.BlockSpec(memory_space=pltpu.VMEM)
    out = pl.pallas_call(
        kernel,
        out_shape=pltpu.VMEM((seq, cols), BF16),
        in_specs=[anyspace] * 7,
        out_specs=vmem,
        scratch_shapes=[
            pltpu.VMEM((1, width), F32),
            pltpu.VMEM(conv_taps.shape, F32),
            pltpu.VMEM((2, seq, width), BF16),
            pltpu.VMEM((2 * seq, width), BF16),
            pltpu.VMEM((3 * (PARTS - 1), width, part), BF16),
            pltpu.VMEM((width, cols), BF16),
            pltpu.VMEM((3, PARTS - 1, 2, seq + PAD, part), BF16),
            pltpu.VMEM((seq, width), BF16),
            pltpu.VMEM((PARTS - 1, seq, part), BF16),
            pltpu.VMEM((seq, cols), F32),
            pltpu.SemaphoreType.DMA((5,)),
            pltpu.SemaphoreType.DMA((COPIES,)),
            pltpu.SemaphoreType.DMA((5,)),
        ],
        compiler_params=pltpu.CompilerParams(
            collective_id=0, has_side_effects=True, vmem_limit_bytes=58 * 1024 * 1024
        ),
        name="mixer",
    )(
        tokens.reshape(seq, width), norm_gain.reshape(1, width), outer_weight, inner_weight,
        value_weight, conv_taps, out_weight,
    )
    return out.reshape(1, seq, cols)


def solution(mesh):
    shape = dict(mesh.shape)

    def local(tokens, *rest):
        rows, cols = rest[1].shape
        fits = (
            shape["fs"] == 4 and shape["tp"] == 2 and shape["rep"] == 4
            and tokens.shape[0] == 1 and tokens.shape[1] % 256 == 0
            and rows % 512 == 0 and cols == 2 * rows and rest[4].shape[0] <= 9
        )
        return (paired if fits else plain)(tokens, *rest)

    in_specs = (
        P(("rep", "fs"), None, None),
        P(),
        P("fs", "tp"),
        P("fs", "tp"),
        P("fs", "tp"),
        P(),
        P("fs", "tp"),
    )
    out_specs = P(("rep", "fs"), None, "tp")
    return jax.shard_map(local, mesh=mesh, in_specs=in_specs, out_specs=out_specs, check_vma=False)
```

```python
import jax
import jax.numpy as jnp
from jax import lax
from jax.experimental import pallas as pl
from jax.experimental.pallas import tpu as pltpu
from jax.sharding import PartitionSpec as P

MESH = pl.DeviceIdType.MESH
F32 = jnp.float32
BF16 = jnp.bfloat16


def plain(tokens, norm_gain, outer_weight, inner_weight, value_weight, conv_taps, out_weight):
    batch, seq_len, width = tokens.shape
    xf = tokens.astype(F32)
    scale = lax.rsqrt(jnp.mean(xf * xf, axis=-1, keepdims=True) + 1e-06)
    normed = (xf * scale * norm_gain).astype(BF16).reshape(batch * seq_len, width)
    columns = outer_weight.shape[1]

    def project(weight):
        full = lax.all_gather(weight, "fs", axis=0, tiled=True)
        return jnp.dot(normed, full, preferred_element_type=F32).astype(BF16).astype(F32)

    outer, inner, value = project(outer_weight), project(inner_weight), project(value_weight)
    product = (inner * value).reshape(batch, seq_len, columns)
    offset = lax.axis_index("tp") * columns
    taps = lax.dynamic_slice_in_dim(conv_taps, offset, columns, 1)
    count = conv_taps.shape[0]
    padded = jnp.pad(product, ((0, 0), (count - 1, 0), (0, 0)))
    convolved = jnp.zeros((batch, seq_len, columns), F32)
    for k in range(count):
        convolved = convolved + taps[k] * padded[:, k : k + seq_len, :]
    gated = (outer * convolved.reshape(batch * seq_len, columns)).astype(BF16)
    everything = lax.all_gather(gated, "tp", axis=1, tiled=True)
    full = lax.all_gather(out_weight, "fs", axis=0, tiled=True)
    result = jnp.dot(everything, full, preferred_element_type=F32)
    return result.astype(BF16).reshape(batch, seq_len, columns)


PARTS = 4
PAD = 16
CROSS = 10
COPIES = CROSS + 31


def kernel(
    tok_hbm, gain_hbm, outer_hbm, inner_hbm, value_hbm, taps_hbm, outw_hbm, out_ref,
    gain_ref, taps_ref, tok, nm, wts, outw, proj, gat, mine, osum, send_sems, recv_sems, local_sems,
):
    rep, fs, tp = lax.axis_index("rep"), lax.axis_index("fs"), lax.axis_index("tp")
    seq, width = tok_hbm.shape
    rows, cols = outer_hbm.shape
    part = cols // PARTS
    hseq = seq // 2
    hrows = rows // 2
    hpart = part // 2
    crows = rows * 6 // 32
    zrows = rows // 8
    orest = hrows - crows
    count = taps_ref.shape[0]
    m = rep // 2
    inner_chip = lax.rem(rep, 2) + m - 2 * lax.rem(rep, 2) * m
    fx = fs + 1 - 2 * lax.rem(fs, 2)
    fy = lax.rem(fs + 2, 4)
    fd = 3 - fs
    fp = fy + m * (fx - fy)
    fq = fx + m * (fy - fx)
    to_x, to_y, to_p, to_q = (rep, fx, tp), (rep, fy, tp), (rep, fp, tp), (rep, fq, tp)
    to_z, to_t = (rep + 1 - 2 * lax.rem(rep, 2), fs, tp), (rep, fs, 1 - tp)
    to_m = (3 - rep, fs, tp)
    cross = {}

    barrier = pltpu.get_barrier_semaphore()
    for peer in (to_x, to_y, to_z, to_t):
        pl.semaphore_signal(barrier, inc=1, device_id=peer, device_id_type=MESH)

    hbm = (inner_hbm, value_hbm, outer_hbm)
    tok_load = pltpu.make_async_copy(tok_hbm, tok.at[0], local_sems.at[0])
    gain_load = pltpu.make_async_copy(gain_hbm, gain_ref, local_sems.at[1])
    taps_load = pltpu.make_async_copy(taps_hbm, taps_ref, local_sems.at[2])
    gain_load.start()
    taps_load.start()
    tok_load.start()

    def al(x, n):
        return pl.multiple_of(x, n)

    tile = 128

    def norm(s, h, halves):
        @pl.loop(0, halves * hseq // tile)
        def _(b):
            r = al(h * hseq + b * tile, tile)
            xf = tok[s, pl.ds(r, tile), :].astype(F32)
            scale = lax.rsqrt(jnp.mean(xf * xf, axis=-1, keepdims=True) + 1e-06)
            nm[pl.ds(al(s * seq + r, tile), tile), :] = (xf * scale * gain_ref[...]).astype(BF16)

    zeros = jnp.zeros((PAD, part), BF16)
    for c in range(PARTS - 1):
        for w in range(2):
            for s in range(2):
                proj[w, c, s, 0:PAD, :] = zeros

    def project(units, blocks):
        b0, nb = blocks[0], len(blocks)
        u0, nu = units[0], len(units)

        @pl.loop(0, nu * nb)
        def _(i):
            u = u0 + i // nb
            b = b0 + lax.rem(i, nb)
            s, h = b // 2, lax.rem(b, 2)
            d = jnp.dot(nm[pl.ds(al(b * hseq, 128), hseq), :], wts[u], preferred_element_type=F32)
            proj[lax.rem(u, 3), u // 3, s, pl.ds(al(PAD + h * hseq, PAD), hseq), :] = d.astype(BF16)

    def gate(c, first, s, h, halves, store):
        tcols = pl.ds(al(tp * cols + first + c * part, 128), part)

        @pl.loop(0, halves * hseq // tile)
        def _(b):
            r = al(h * hseq + b * tile, tile)
            inner = proj[0, c, s, pl.ds(r, tile + PAD), :].astype(F32)
            value = proj[1, c, s, pl.ds(r, tile + PAD), :].astype(F32)
            outer = proj[2, c, s, pl.ds(al(r + PAD, PAD), tile), :].astype(F32)
            window = inner * value
            conv = jnp.zeros((tile, part), F32)
            for k in range(count):
                lo = PAD - (count - 1) + k
                conv = conv + taps_ref[k : k + 1, tcols] * window[lo : lo + tile, :]
            store(pl.ds(r, tile), (outer * conv).astype(BF16))

    def mix(h, terms, first, last):
        r = slice(0, seq) if h is None else slice(h * hseq, (h + 1) * hseq)

        for b in range(cols // part):
            at = slice(b * part, (b + 1) * part)
            total = None
            for k, n in terms:
                d = jnp.dot(gat[r, pl.ds(k, n)], outw[pl.ds(k, n), at], preferred_element_type=F32)
                total = d if total is None else total + d
            if not first:
                total = total + osum[r, at]
            if last:
                out_ref[r, at] = total.astype(BF16)
            else:
                osum[r, at] = total

    def program(inside):
        local = {}

        def index(key):
            if key[0] in ("tz", "gz", "ge", "oz"):
                return cross.setdefault(key, len(cross))
            return CROSS + local.setdefault(key, len(local))

        def send(key, src, dst, device, group):
            k = index(key)
            pltpu.make_async_remote_copy(
                src_ref=src, dst_ref=dst, send_sem=send_sems.at[group], recv_sem=recv_sems.at[k],
                device_id=device, device_id_type=MESH,
            ).start()

        def wait(key, dst):
            k = index(key)
            pltpu.make_async_remote_copy(
                src_ref=dst, dst_ref=dst, send_sem=send_sems.at[0], recv_sem=recv_sems.at[k],
                device_id=to_t, device_id_type=MESH,
            ).wait_recv()

        def wait_sent(group, src):
            pltpu.make_async_remote_copy(
                src_ref=src, dst_ref=src, send_sem=send_sems.at[group], recv_sem=recv_sems.at[0],
                device_id=to_t, device_id_type=MESH,
            ).wait_send()

        chunks = PARTS - 1 if inside else 2
        first = part if inside else 0
        units = 3 * chunks

        def split(c):
            return c == (0 if inside else 1)

        def widths(c, act):
            if not split(c):
                act(0, part)
                return
            pl.when(tp == 0)(lambda: act(hpart if inside else 0, hpart))
            if inside:
                pl.when(tp == 1)(lambda: act(0, part))

        for u in range(units):
            c, w = u // 3, u % 3
            pltpu.make_async_copy(
                hbm[w].at[:, pl.ds(first + c * part, part)],
                wts.at[u, pl.ds(al(fs * rows, rows), rows)], local_sems.at[3],
            ).start()
        w_load = pltpu.make_async_copy(
            wts.at[0:units, 0:rows], wts.at[0:units, 0:rows], local_sems.at[3])
        ow_load = pltpu.make_async_copy(
            outw_hbm, outw.at[pl.ds(al(fs * rows, rows), rows)], local_sems.at[4])
        ow_load.start()

        def wrow(u, f, off, n, lo, wd):
            return wts.at[u, pl.ds(al(f * rows + off, 128), n), pl.ds(lo, wd)]

        def orow(f, off, n):
            return outw.at[pl.ds(al(f * rows + off, 16), n)]

        def trow(h, t):
            return pl.ds(al(h * hseq + t * (hseq // 2), 64), hseq // 2)

        def tok_z(h):
            send(("tz", h), tok_hbm.at[trow(h, tp)], tok.at[1, trow(h, tp)], to_z, 1)

        def tok_f(h):
            here = tok.at[1, trow(h, tp)]
            wait(("tz", h), here)
            send(("tt", h), here, here, to_t, 1)

        def tok_w(h):
            wait(("tt", h), tok.at[1, trow(h, 1 - tp)])

        def gcols(c, lo, wd):
            return pl.ds(al(tp * cols + first + c * part + lo, 128), wd)

        def grow(h):
            return pl.ds(0, seq) if h is None else pl.ds(h * hseq, hseq)

        def own_gate(c, key):
            def store(r, x):
                def act(lo, wd):
                    gat[r, gcols(c, lo, wd)] = x[:, lo : lo + wd]
                widths(c, act)

            def out(lo, wd):
                here = gat.at[:, gcols(c, lo, wd)]
                send(key, here, here, to_t, 3)

            def run():
                gate(c, first, 0, 0, 2, store)
                widths(c, out)

            if split(c) and not inside:
                pl.when(tp == 0)(run)
            else:
                run()

        def partner_gate(c, h):
            key = ("gz", c, h if c == PARTS - 2 else None) if inside else ("ge",)

            def store(r, x):
                mine[c, r, :] = x

            def out(lo, wd):
                src = mine.at[c, grow(h), pl.ds(lo, wd)]
                send(key, src, gat.at[grow(h), gcols(c, lo, wd)], to_z, 3)

            def run():
                gate(c, first, 1, h or 0, 2 if h is None else 1, store)
                widths(c, out)

            if split(c) and not inside:
                pl.when(tp == 0)(run)
            else:
                run()

        def forward(key, h, at, wd, new):
            here = gat.at[grow(h), pl.ds(al(tp * cols + at, 128), wd)]
            wait(key, here)
            send(new, here, here, to_t, 3)

        def take_other(key, h, parts):
            wait(key, gat.at[grow(h), pl.ds(0, parts * part)])

        f_off, g_off = m * hrows, (1 - m) * hrows
        c_off, o_off = g_off + (1 - m) * orest, g_off + m * crows
        zp_off, zq_off = g_off + m * (hrows - zrows), f_off + (1 - m) * (hrows - zrows)

        def krow(f, off):
            return al(f * rows + off, 128), hrows


        if inside:
            pl.semaphore_signal(barrier, inc=1, device_id=to_m, device_id_type=MESH)
            pl.semaphore_wait(barrier, 5)
            hx, hy = m * hrows, (1 - m) * hrows

            def direct(u):
                c, w = u // 3, u % 3

                def act(lo, wd):
                    at = pl.ds(first + c * part + lo, wd)
                    for off, to in ((hx, to_x), (hy, to_y)):
                        src = hbm[w].at[pl.ds(al(off, 128), hrows), at]
                        send(("d", u), src, wrow(u, fs, off, hrows, lo, wd), to, 0)
                widths(c, act)

            def relay(u):
                def act(lo, wd):
                    wait(("d", u), wts.at[u, 0 : 2 * hrows, lo : lo + wd])
                    bx, by = wrow(u, fx, hx, hrows, lo, wd), wrow(u, fy, hy, hrows, lo, wd)
                    send(("r", u), bx, bx, to_m, 0)
                    send(("r", u), by, by, to_x, 0)
                    send(("r", u), bx, bx, to_y, 0)
                    send(("r", u), by, by, to_m, 0)
                widths(u // 3, act)

            def ready(u):
                if u == 0:
                    w_load.wait()
                widths(u // 3, lambda lo, wd: wait(("r", u), wts.at[u, 0 : 4 * hrows, lo : lo + wd]))

            def out_rows(key, off, n, to):
                send(key, outw_hbm.at[pl.ds(al(off, 16), n)], orow(fs, off, n), to, 2)

            tok_z(0)
            tok_z(1)
            for u in range(3):
                direct(u)
            tok_load.wait()
            gain_load.wait()
            norm(0, 0, 2)
            relay(0)
            direct(3)
            relay(1)
            direct(4)
            relay(2)
            direct(5)
            ready(0)
            project([0], [0, 1])
            relay(3)
            direct(6)
            out_rows(("oe",), zp_off, zrows, to_p)
            out_rows(("oe",), zq_off, zrows, to_q)
            ready(1)
            project([1], [0, 1])
            tok_f(0)
            relay(4)
            direct(7)
            tok_w(0)
            norm(1, 0, 1)
            ready(2)
            project([2], [0, 1])
            project([0, 1, 2], [2])
            taps_load.wait()
            partner_gate(0, 0)
            own_gate(0, ("ga",))
            relay(5)
            direct(8)
            ready(3)
            project([3], [0, 1, 2])
            relay(6)
            wait(("oe",), outw.at[0 : 2 * zrows])
            for f, off in ((fp, zp_off), (fq, zq_off)):
                block = orow(f, off, zrows)
                send(("oz", 2), block, block, to_z, 2)
            ready(4)
            tok_f(1)
            project([4], [0, 1, 2])
            relay(7)
            tok_w(1)
            norm(1, 1, 1)
            project([0, 1, 2], [3])
            partner_gate(0, 1)
            relay(8)
            out_rows(("o", 0), f_off, hrows, to_p)
            out_rows(("o", 0), f_off + m * zrows, hrows - zrows, to_q)
            out_rows(("o", 1), o_off + (1 - m) * zrows, orest - zrows, to_p)
            out_rows(("o", 1), o_off, orest, to_q)
            ready(5)
            project([5], [0, 1, 2])
            partner_gate(1, 0)
            project([3, 4, 5], [3])
            partner_gate(1, 1)
            own_gate(1, ("ga",))
            wait(("oz", 0), orow(fd, f_off, hrows))

            def swap():
                block = orow(fd, f_off, hrows)
                send(("om",), block, block, to_m, 2)

            pl.when(tp == 0)(swap)
            ready(6)
            project([6], [0, 1, 2, 3])
            ready(7)
            project([7], [0, 1, 2, 3])
            ready(8)
            project([8], [2])
            partner_gate(2, 0)
            project([8], [3])
            partner_gate(2, 1)
            pl.when(tp == 1)(swap)
            project([8], [0, 1])
            own_gate(2, ("ga",))
            pl.when(tp == 0)(lambda: forward(("ge",), None, 0, part + hpart, ("ga",)))
            pl.when(tp == 1)(lambda: forward(("ge",), None, 0, part, ("ga",)))
            ow_load.wait()
            take_other(("ga",), None, PARTS)
            mix(None, [(al(fs * rows, rows), rows), krow(fd, f_off)], True, False)
            wait(("o", 0), outw.at[0 : 2 * hrows - zrows])
            mix(None, [krow(fx, f_off), krow(fy, f_off)], False, False)
            wait(("om",), orow(fd, g_off, hrows))
            mix(None, [krow(fd, g_off)], False, False)
            wait(("oz", 1), outw.at[0 : 2 * crows])
            wait(("o", 1), outw.at[0 : 2 * orest - zrows])
            mix(None, [krow(fx, g_off), krow(fy, g_off)], False, True)
            pl.when(tp == 0)(lambda: wait_sent(0, wts.at[:, 0 : 5 * hrows]))
            pl.when(tp == 1)(lambda: wait_sent(0, wts.at[:, 0 : 6 * hrows]))
            wait_sent(1, tok.at[0])
            wait_sent(2, outw.at[0 : 3 * hrows + 2 * orest + 2 * zrows])
            pl.when(tp == 0)(lambda: wait_sent(3, gat.at[:, 0 : 13 * hpart]))
            pl.when(tp == 1)(lambda: wait_sent(3, gat.at[:, 0 : 14 * hpart]))
        else:
            pl.semaphore_wait(barrier, 4)

            def direct(u, which):
                c, w = u // 3, u % 3
                wd = hpart if split(c) else part
                src = hbm[w].at[:, pl.ds(first + c * part, wd)]
                send(("d" + which, u), src, wrow(u, fs, 0, rows, 0, wd), to_p if which == "p" else to_q, 0)

            def relay_q(u):
                wd = hpart if split(u // 3) else part
                wait(("dp", u), wrow(u, fp, 0, rows, 0, wd))
                block = wrow(u, fp, f_off, hrows, 0, wd)
                send(("r", u), block, block, to_q, 0)

            def relay_p(u):
                wd = hpart if split(u // 3) else part
                wait(("dq", u), wrow(u, fq, 0, rows, 0, wd))
                block = wrow(u, fq, g_off, hrows, 0, wd)
                send(("r", u), block, block, to_p, 0)

            def ready(u):
                if u == 0:
                    w_load.wait()
                wd = hpart if split(u // 3) else part
                wait(("r", u), wts.at[u, 0 : 2 * hrows, 0:wd])

            def out_rows(key, off, n, to):
                send(key, outw_hbm.at[pl.ds(al(off, 16), n)], orow(fs, off, n), to, 2)

            extra = pl.when(tp == 0)

            tok_z(0)
            tok_z(1)
            out_rows(("op", 0), f_off, hrows, to_p)
            for u in range(3):
                direct(u, "q")
                direct(u, "p")

            @extra
            def _():
                for u in range(3, 6):
                    direct(u, "p")

            tok_load.wait()
            gain_load.wait()
            norm(0, 0, 2)
            relay_p(0)
            relay_p(1)
            block = orow(fp, f_off, hrows)
            wait(("op", 0), block)
            send(("orq",), block, block, to_q, 2)

            @extra
            def _():
                for u in range(3, 6):
                    direct(u, "q")


            relay_p(2)
            relay_q(0)
            tok_f(0)
            relay_q(1)
            tok_w(0)
            norm(1, 0, 1)
            relay_q(2)
            block = orow(fd, f_off, hrows)
            wait(("orq",), block)
            send(("oz", 0), block, block, to_z, 2)

            tok_f(1)
            ready(0)
            project([0], [0, 1, 2])

            @extra
            def _():
                for u in range(3, 6):
                    relay_p(u)
                    relay_q(u)

            ready(1)
            project([1], [0, 1, 2])
            out_rows(("op", 1), g_off + (1 - m) * zrows, hrows - zrows, to_p)
            for b in range(2):
                out_rows(("oq", b), g_off + b * hrows // 2, hrows // 2, to_q)
            def last_rows():
                out_rows(("oq", 2), f_off + m * zrows, hrows - zrows, to_q)

            extra(last_rows)
            tok_w(1)
            norm(1, 1, 1)
            ready(2)
            taps_load.wait()
            project([2], [2])
            project([0, 1, 2], [3])
            partner_gate(0, None)

            @extra
            def _():
                for u in range(3, 6):
                    ready(u)
                project([3, 4, 5], [2, 3])
            partner_gate(1, None)
            def pass_on(b):
                block = orow(fq, g_off + b * hrows // 2, hrows // 2)
                wait(("oq", b), block)
                send(("orp",), block, block, to_p, 2)

            project([2], [0, 1])
            own_gate(0, ("ga",))
            pass_on(0)
            extra(lambda: project([3, 4], [0, 1]))
            wait(("op", 1), orow(fp, g_off, hrows - zrows))
            block = orow(fp, c_off, crows)
            send(("oz", 1), block, block, to_z, 4)
            extra(lambda: project([5], [0, 1]))
            own_gate(1, ("ga",))
            pl.when(tp == 0)(lambda: forward(("gz", 0, None), None, part + hpart, hpart, ("ga",)))
            pl.when(tp == 1)(lambda: forward(("gz", 0, None), None, part, part, ("ga",)))
            pass_on(1)
            pl.when(tp == 1)(last_rows)
            block = orow(fq, c_off, crows)
            send(("oz", 1), block, block, to_z, 4)
            forward(("gz", 1, None), None, 2 * part, part, ("gb",))
            ow_load.wait()
            take_other(("ga",), None, 2)
            take_other(("gb",), None, 1)
            wait(("oz", 2), outw.at[0 : 2 * zrows])
            odd = lax.rem(fs, 2)
            mix(None, [krow(fs, 0), krow(fp, 0), krow(fd + m * (fq - fd), 0),
                       krow(fs + odd * (fx - fs), hrows)], True, False)
            for h in range(2):
                forward(("gz", 2, h), h, 3 * part, part, ("gc", h))
            wait(("oq", 2), orow(fq, f_off, hrows - zrows))
            late = [krow(fq, f_off), krow(fp + m * (fd - fp), hrows), krow(fx + odd * (fs - fx), hrows)]
            take_other(("gc", 0), 0, 1)
            mix(0, late, False, False)
            wait(("orp",), orow(fd, g_off, hrows))
            mix(0, [krow(fd, g_off)], False, True)
            take_other(("gc", 1), 1, 1)
            mix(1, late + [krow(fd, g_off)], False, True)
            pl.when(tp == 0)(lambda: wait_sent(0, wts.at[0:6, 0 : 9 * hrows // 2]))
            pl.when(tp == 1)(lambda: wait_sent(0, wts.at[0:3, 0 : 6 * hrows]))
            wait_sent(1, tok.at[0])
            wait_sent(2, outw.at[0 : 7 * hrows - 2 * zrows])
            pl.when(tp == 0)(lambda: wait_sent(3, gat.at[:, 0 : 11 * hpart]))
            pl.when(tp == 1)(lambda: wait_sent(3, gat.at[:, 0 : 10 * hpart]))
            wait_sent(4, outw.at[0 : 2 * crows])

    @pl.when(inner_chip == 1)
    def _():
        program(True)

    @pl.when(inner_chip == 0)
    def _():
        program(False)

    assert len(cross) <= CROSS


def paired(tokens, norm_gain, outer_weight, inner_weight, value_weight, conv_taps, out_weight):
    _, seq, width = tokens.shape
    rows, cols = outer_weight.shape
    part = cols // PARTS
    anyspace = pl.BlockSpec(memory_space=pltpu.HBM)
    vmem = pl.BlockSpec(memory_space=pltpu.VMEM)
    out = pl.pallas_call(
        kernel,
        out_shape=pltpu.VMEM((seq, cols), BF16),
        in_specs=[anyspace] * 7,
        out_specs=vmem,
        scratch_shapes=[
            pltpu.VMEM((1, width), F32),
            pltpu.VMEM(conv_taps.shape, F32),
            pltpu.VMEM((2, seq, width), BF16),
            pltpu.VMEM((2 * seq, width), BF16),
            pltpu.VMEM((3 * (PARTS - 1), width, part), BF16),
            pltpu.VMEM((width, cols), BF16),
            pltpu.VMEM((3, PARTS - 1, 2, seq + PAD, part), BF16),
            pltpu.VMEM((seq, width), BF16),
            pltpu.VMEM((PARTS - 1, seq, part), BF16),
            pltpu.VMEM((seq, cols), F32),
            pltpu.SemaphoreType.DMA((5,)),
            pltpu.SemaphoreType.DMA((COPIES,)),
            pltpu.SemaphoreType.DMA((5,)),
        ],
        compiler_params=pltpu.CompilerParams(
            collective_id=0, has_side_effects=True, vmem_limit_bytes=58 * 1024 * 1024
        ),
        name="mixer",
    )(
        tokens.reshape(seq, width), norm_gain.reshape(1, width), outer_weight, inner_weight,
        value_weight, conv_taps, out_weight,
    )
    return out.reshape(1, seq, cols)


def solution(mesh):
    shape = dict(mesh.shape)

    def local(tokens, *rest):
        rows, cols = rest[1].shape
        fits = (
            shape["fs"] == 4 and shape["tp"] == 2 and shape["rep"] == 4
            and tokens.shape[0] == 1 and tokens.shape[1] % 256 == 0
            and rows % 512 == 0 and cols == 2 * rows and rest[4].shape[0] <= 9
        )
        return (paired if fits else plain)(tokens, *rest)

    in_specs = (
        P(("rep", "fs"), None, None),
        P(),
        P("fs", "tp"),
        P("fs", "tp"),
        P("fs", "tp"),
        P(),
        P("fs", "tp"),
    )
    out_specs = P(("rep", "fs"), None, "tp")
    return jax.shard_map(local, mesh=mesh, in_specs=in_specs, out_specs=out_specs, check_vma=False)
```

```python
import jax
import jax.numpy as jnp
from jax import lax
from jax.experimental import pallas as pl
from jax.experimental.pallas import tpu as pltpu
from jax.sharding import PartitionSpec as P

MESH = pl.DeviceIdType.MESH
F32 = jnp.float32
BF16 = jnp.bfloat16


def plain(tokens, norm_gain, outer_weight, inner_weight, value_weight, conv_taps, out_weight):
    batch, seq_len, width = tokens.shape
    xf = tokens.astype(F32)
    scale = lax.rsqrt(jnp.mean(xf * xf, axis=-1, keepdims=True) + 1e-06)
    normed = (xf * scale * norm_gain).astype(BF16).reshape(batch * seq_len, width)
    columns = outer_weight.shape[1]

    def project(weight):
        full = lax.all_gather(weight, "fs", axis=0, tiled=True)
        return jnp.dot(normed, full, preferred_element_type=F32).astype(BF16).astype(F32)

    outer, inner, value = project(outer_weight), project(inner_weight), project(value_weight)
    product = (inner * value).reshape(batch, seq_len, columns)
    offset = lax.axis_index("tp") * columns
    taps = lax.dynamic_slice_in_dim(conv_taps, offset, columns, 1)
    count = conv_taps.shape[0]
    padded = jnp.pad(product, ((0, 0), (count - 1, 0), (0, 0)))
    convolved = jnp.zeros((batch, seq_len, columns), F32)
    for k in range(count):
        convolved = convolved + taps[k] * padded[:, k : k + seq_len, :]
    gated = (outer * convolved.reshape(batch * seq_len, columns)).astype(BF16)
    everything = lax.all_gather(gated, "tp", axis=1, tiled=True)
    full = lax.all_gather(out_weight, "fs", axis=0, tiled=True)
    result = jnp.dot(everything, full, preferred_element_type=F32)
    return result.astype(BF16).reshape(batch, seq_len, columns)


PARTS = 4
PAD = 16
CROSS = 10
COPIES = CROSS + 25


def kernel(
    tok_hbm, gain_hbm, outer_hbm, inner_hbm, value_hbm, taps_hbm, outw_hbm, out_ref,
    gain_ref, taps_ref, tok, nm, wts, outw, proj, gat, mine, osum, send_sems, recv_sems, local_sems,
):
    rep, fs, tp = lax.axis_index("rep"), lax.axis_index("fs"), lax.axis_index("tp")
    seq, width = tok_hbm.shape
    rows, cols = outer_hbm.shape
    part = cols // PARTS
    hseq = seq // 2
    hrows = rows // 2
    hpart = part // 2
    crows = rows * 6 // 32
    zrows = rows // 8
    orest = hrows - crows
    count = taps_ref.shape[0]
    m = rep // 2
    inner_chip = lax.rem(rep, 2) + m - 2 * lax.rem(rep, 2) * m
    fx = fs + 1 - 2 * lax.rem(fs, 2)
    fy = lax.rem(fs + 2, 4)
    fd = 3 - fs
    fp = fy + m * (fx - fy)
    fq = fx + m * (fy - fx)
    to_x, to_y, to_p, to_q = (rep, fx, tp), (rep, fy, tp), (rep, fp, tp), (rep, fq, tp)
    to_z, to_t = (rep + 1 - 2 * lax.rem(rep, 2), fs, tp), (rep, fs, 1 - tp)
    to_m = (3 - rep, fs, tp)
    cross = {}

    barrier = pltpu.get_barrier_semaphore()
    for peer in (to_x, to_y, to_z, to_t):
        pl.semaphore_signal(barrier, inc=1, device_id=peer, device_id_type=MESH)

    hbm = (inner_hbm, value_hbm, outer_hbm)
    tok_load = pltpu.make_async_copy(tok_hbm, tok.at[0], local_sems.at[0])
    gain_load = pltpu.make_async_copy(gain_hbm, gain_ref, local_sems.at[1])
    taps_load = pltpu.make_async_copy(taps_hbm, taps_ref, local_sems.at[2])
    gain_load.start()
    taps_load.start()
    tok_load.start()

    def al(x, n):
        return pl.multiple_of(x, n)

    tile = 128

    def norm(s, h, halves):
        @pl.loop(0, halves * hseq // tile)
        def _(b):
            r = al(h * hseq + b * tile, tile)
            xf = tok[s, pl.ds(r, tile), :].astype(F32)
            scale = lax.rsqrt(jnp.mean(xf * xf, axis=-1, keepdims=True) + 1e-06)
            nm[pl.ds(al(s * seq + r, tile), tile), :] = (xf * scale * gain_ref[...]).astype(BF16)

    zeros = jnp.zeros((PAD, part), BF16)
    for c in range(PARTS - 1):
        for w in range(2):
            for s in range(2):
                proj[w, c, s, 0:PAD, :] = zeros

    def project(units, blocks):
        b0, nb = blocks[0], len(blocks)
        u0, nu = units[0], len(units)

        @pl.loop(0, nu * nb)
        def _(i):
            u = u0 + i // nb
            b = b0 + lax.rem(i, nb)
            s, h = b // 2, lax.rem(b, 2)
            d = jnp.dot(nm[pl.ds(al(b * hseq, 128), hseq), :], wts[u], preferred_element_type=F32)
            proj[lax.rem(u, 3), u // 3, s, pl.ds(al(PAD + h * hseq, PAD), hseq), :] = d.astype(BF16)

    def gate(c, first, s, h, halves, store):
        tcols = pl.ds(al(tp * cols + first + c * part, 128), part)

        @pl.loop(0, halves * hseq // tile)
        def _(b):
            r = al(h * hseq + b * tile, tile)
            inner = proj[0, c, s, pl.ds(r, tile + PAD), :].astype(F32)
            value = proj[1, c, s, pl.ds(r, tile + PAD), :].astype(F32)
            outer = proj[2, c, s, pl.ds(al(r + PAD, PAD), tile), :].astype(F32)
            window = inner * value
            conv = jnp.zeros((tile, part), F32)
            for k in range(count):
                lo = PAD - (count - 1) + k
                conv = conv + taps_ref[k : k + 1, tcols] * window[lo : lo + tile, :]
            store(pl.ds(r, tile), (outer * conv).astype(BF16))

    def mix(h, terms, first, last):
        r = slice(0, seq) if h is None else slice(h * hseq, (h + 1) * hseq)

        for b in range(cols // part):
            at = slice(b * part, (b + 1) * part)
            total = None
            for k, n in terms:
                d = jnp.dot(gat[r, pl.ds(k, n)], outw[pl.ds(k, n), at], preferred_element_type=F32)
                total = d if total is None else total + d
            if not first:
                total = total + osum[r, at]
            if last:
                out_ref[r, at] = total.astype(BF16)
            else:
                osum[r, at] = total

    def program(inside):
        local = {}

        def index(key):
            if key[0] in ("tz", "gz", "ge", "oz"):
                return cross.setdefault(key, len(cross))
            return CROSS + local.setdefault(key, len(local))

        def send(key, src, dst, device, group):
            k = index(key)
            pltpu.make_async_remote_copy(
                src_ref=src, dst_ref=dst, send_sem=send_sems.at[group], recv_sem=recv_sems.at[k],
                device_id=device, device_id_type=MESH,
            ).start()

        def wait(key, dst):
            k = index(key)
            pltpu.make_async_remote_copy(
                src_ref=dst, dst_ref=dst, send_sem=send_sems.at[0], recv_sem=recv_sems.at[k],
                device_id=to_t, device_id_type=MESH,
            ).wait_recv()

        def wait_sent(group, src):
            pltpu.make_async_remote_copy(
                src_ref=src, dst_ref=src, send_sem=send_sems.at[group], recv_sem=recv_sems.at[0],
                device_id=to_t, device_id_type=MESH,
            ).wait_send()

        chunks = PARTS - 1 if inside else 2
        first = part if inside else 0
        units = 3 * chunks

        def split(c):
            return c == (0 if inside else 1)

        def widths(c, act):
            if not split(c):
                act(0, part)
                return
            pl.when(tp == 0)(lambda: act(hpart if inside else 0, hpart))
            if inside:
                pl.when(tp == 1)(lambda: act(0, part))

        for u in range(units):
            c, w = u // 3, u % 3
            pltpu.make_async_copy(
                hbm[w].at[:, pl.ds(first + c * part, part)],
                wts.at[u, pl.ds(al(fs * rows, rows), rows)], local_sems.at[3],
            ).start()
        w_load = pltpu.make_async_copy(
            wts.at[0:units, 0:rows], wts.at[0:units, 0:rows], local_sems.at[3])
        ow_load = pltpu.make_async_copy(
            outw_hbm, outw.at[pl.ds(al(fs * rows, rows), rows)], local_sems.at[4])
        ow_load.start()

        def wrow(u, f, off, n, lo, wd):
            return wts.at[u, pl.ds(al(f * rows + off, 128), n), pl.ds(lo, wd)]

        def orow(f, off, n):
            return outw.at[pl.ds(al(f * rows + off, 16), n)]

        def trow(h, t):
            return pl.ds(al(h * hseq + t * (hseq // 2), 64), hseq // 2)

        def tok_z(h):
            send(("tz", h), tok_hbm.at[trow(h, tp)], tok.at[1, trow(h, tp)], to_z, 1)

        def tok_f(h):
            here = tok.at[1, trow(h, tp)]
            wait(("tz", h), here)
            send(("tt", h), here, here, to_t, 1)

        def tok_w(h):
            wait(("tt", h), tok.at[1, trow(h, 1 - tp)])

        def gcols(c, lo, wd):
            return pl.ds(al(tp * cols + first + c * part + lo, 128), wd)

        def grow(h):
            return pl.ds(0, seq) if h is None else pl.ds(h * hseq, hseq)

        def own_gate(c, key):
            def store(r, x):
                def act(lo, wd):
                    gat[r, gcols(c, lo, wd)] = x[:, lo : lo + wd]
                widths(c, act)

            def out(lo, wd):
                here = gat.at[:, gcols(c, lo, wd)]
                send(key, here, here, to_t, 3)

            def run():
                gate(c, first, 0, 0, 2, store)
                widths(c, out)

            if split(c) and not inside:
                pl.when(tp == 0)(run)
            else:
                run()

        def partner_gate(c, h):
            key = ("gz", c, h if c == PARTS - 2 else None) if inside else ("ge",)

            def store(r, x):
                mine[c, r, :] = x

            def out(lo, wd):
                src = mine.at[c, grow(h), pl.ds(lo, wd)]
                send(key, src, gat.at[grow(h), gcols(c, lo, wd)], to_z, 3)

            def run():
                gate(c, first, 1, h or 0, 2 if h is None else 1, store)
                widths(c, out)

            if split(c) and not inside:
                pl.when(tp == 0)(run)
            else:
                run()

        def forward(key, h, at, wd, new):
            here = gat.at[grow(h), pl.ds(al(tp * cols + at, 128), wd)]
            wait(key, here)
            send(new, here, here, to_t, 3)

        def take_other(key, h, parts):
            wait(key, gat.at[grow(h), pl.ds(0, parts * part)])

        f_off, g_off = m * hrows, (1 - m) * hrows
        c_off, o_off = g_off + (1 - m) * orest, g_off + m * crows
        zp_off, zq_off = g_off + m * (hrows - zrows), f_off + (1 - m) * (hrows - zrows)

        def krow(f, off):
            return al(f * rows + off, 128), hrows


        if inside:
            pl.semaphore_signal(barrier, inc=1, device_id=to_m, device_id_type=MESH)
            pl.semaphore_wait(barrier, 5)
            hx, hy = m * hrows, (1 - m) * hrows

            def direct(u):
                c, w = u // 3, u % 3

                def act(lo, wd):
                    at = pl.ds(first + c * part + lo, wd)
                    for off, to in ((hx, to_x), (hy, to_y)):
                        src = hbm[w].at[pl.ds(al(off, 128), hrows), at]
                        send(("d", u), src, wrow(u, fs, off, hrows, lo, wd), to, 0)
                widths(c, act)

            def relay(u):
                def act(lo, wd):
                    wait(("d", u), wts.at[u, 0 : 2 * hrows, lo : lo + wd])
                    bx, by = wrow(u, fx, hx, hrows, lo, wd), wrow(u, fy, hy, hrows, lo, wd)
                    send(("r", u), bx, bx, to_m, 0)
                    send(("r", u), by, by, to_x, 0)
                    send(("r", u), bx, bx, to_y, 0)
                    send(("r", u), by, by, to_m, 0)
                widths(u // 3, act)

            def ready(u):
                if u == 0:
                    w_load.wait()
                widths(u // 3, lambda lo, wd: wait(("r", u), wts.at[u, 0 : 4 * hrows, lo : lo + wd]))

            def out_rows(key, off, n, to):
                send(key, outw_hbm.at[pl.ds(al(off, 16), n)], orow(fs, off, n), to, 2)

            tok_z(0)
            tok_z(1)
            for u in range(3):
                direct(u)
            tok_load.wait()
            gain_load.wait()
            norm(0, 0, 2)
            relay(0)
            direct(3)
            relay(1)
            direct(4)
            relay(2)
            direct(5)
            ready(0)
            project([0], [0, 1])
            relay(3)
            direct(6)
            out_rows(("oe",), zp_off, zrows, to_p)
            out_rows(("oe",), zq_off, zrows, to_q)
            ready(1)
            project([1], [0, 1])
            tok_f(0)
            relay(4)
            direct(7)
            tok_w(0)
            norm(1, 0, 1)
            ready(2)
            project([2], [0, 1])
            project([0, 1, 2], [2])
            taps_load.wait()
            partner_gate(0, 0)
            own_gate(0, ("ga",))
            relay(5)
            direct(8)
            ready(3)
            project([3], [0, 1, 2])
            relay(6)
            wait(("oe",), outw.at[0 : 2 * zrows])
            for f, off in ((fp, zp_off), (fq, zq_off)):
                block = orow(f, off, zrows)
                send(("oz", 2), block, block, to_z, 2)
            ready(4)
            tok_f(1)
            project([4], [0, 1, 2])
            relay(7)
            tok_w(1)
            norm(1, 1, 1)
            project([0, 1, 2], [3])
            partner_gate(0, 1)
            relay(8)
            out_rows(("o", 0), f_off, hrows, to_p)
            out_rows(("o", 0), f_off + m * zrows, hrows - zrows, to_q)
            out_rows(("o", 1), o_off + (1 - m) * zrows, orest - zrows, to_p)
            out_rows(("o", 1), o_off, orest, to_q)
            ready(5)
            project([5], [0, 1, 2])
            partner_gate(1, 0)
            project([3, 4, 5], [3])
            partner_gate(1, 1)
            own_gate(1, ("ga",))
            wait(("oz", 0), orow(fd, f_off, hrows))

            def swap():
                block = orow(fd, f_off, hrows)
                send(("om",), block, block, to_m, 2)

            pl.when(tp == 0)(swap)
            ready(6)
            project([6], [0, 1, 2, 3])
            ready(7)
            project([7], [0, 1, 2, 3])
            ready(8)
            project([8], [2])
            partner_gate(2, 0)
            project([8], [3])
            partner_gate(2, 1)
            pl.when(tp == 1)(swap)
            project([8], [0, 1])
            own_gate(2, ("ga",))
            pl.when(tp == 0)(lambda: forward(("ge",), None, 0, part + hpart, ("ga",)))
            pl.when(tp == 1)(lambda: forward(("ge",), None, 0, part, ("ga",)))
            ow_load.wait()
            take_other(("ga",), None, PARTS)
            mix(None, [(al(fs * rows, rows), rows), krow(fd, f_off)], True, False)
            wait(("o", 0), outw.at[0 : 2 * hrows - zrows])
            mix(None, [krow(fx, f_off), krow(fy, f_off)], False, False)
            wait(("om",), orow(fd, g_off, hrows))
            mix(None, [krow(fd, g_off)], False, False)
            wait(("oz", 1), outw.at[0 : 2 * crows])
            wait(("o", 1), outw.at[0 : 2 * orest - zrows])
            mix(None, [krow(fx, g_off), krow(fy, g_off)], False, True)
            pl.when(tp == 0)(lambda: wait_sent(0, wts.at[:, 0 : 5 * hrows]))
            pl.when(tp == 1)(lambda: wait_sent(0, wts.at[:, 0 : 6 * hrows]))
            wait_sent(1, tok.at[0])
            wait_sent(2, outw.at[0 : 3 * hrows + 2 * orest + 2 * zrows])
            pl.when(tp == 0)(lambda: wait_sent(3, gat.at[:, 0 : 13 * hpart]))
            pl.when(tp == 1)(lambda: wait_sent(3, gat.at[:, 0 : 14 * hpart]))
        else:
            pl.semaphore_wait(barrier, 4)

            def direct(u, which):
                c, w = u // 3, u % 3
                wd = hpart if split(c) else part
                src = hbm[w].at[:, pl.ds(first + c * part, wd)]
                send(("d" + which, min(u, 3)), src, wrow(u, fs, 0, rows, 0, wd), to_p if which == "p" else to_q, 0)

            def relay_q(u):
                wd = hpart if split(u // 3) else part
                if u < 3:
                    wait(("dp", u), wrow(u, fp, 0, rows, 0, wd))
                block = wrow(u, fp, f_off, hrows, 0, wd)
                send(("r", min(u, 3)), block, block, to_q, 0)

            def relay_p(u):
                wd = hpart if split(u // 3) else part
                if u < 3:
                    wait(("dq", u), wrow(u, fq, 0, rows, 0, wd))
                block = wrow(u, fq, g_off, hrows, 0, wd)
                send(("r", min(u, 3)), block, block, to_p, 0)

            def ready(u):
                if u == 0:
                    w_load.wait()
                wd = hpart if split(u // 3) else part
                wait(("r", u), wts.at[u, 0 : 2 * hrows, 0:wd])

            def out_rows(key, off, n, to):
                send(key, outw_hbm.at[pl.ds(al(off, 16), n)], orow(fs, off, n), to, 2)

            extra = pl.when(tp == 0)

            tok_z(0)
            tok_z(1)
            out_rows(("op", 0), f_off, hrows, to_p)
            for u in range(3):
                direct(u, "q")
                direct(u, "p")

            @extra
            def _():
                for u in range(3, 6):
                    direct(u, "p")

            tok_load.wait()
            gain_load.wait()
            norm(0, 0, 2)
            relay_p(0)
            relay_p(1)
            block = orow(fp, f_off, hrows)
            wait(("op", 0), block)
            send(("orq",), block, block, to_q, 2)

            @extra
            def _():
                for u in range(3, 6):
                    direct(u, "q")


            relay_p(2)
            relay_q(0)
            tok_f(0)
            relay_q(1)
            tok_w(0)
            norm(1, 0, 1)
            relay_q(2)
            block = orow(fd, f_off, hrows)
            wait(("orq",), block)
            send(("oz", 0), block, block, to_z, 2)

            tok_f(1)
            ready(0)
            project([0], [0, 1, 2])

            @extra
            def _():
                wait(("dq", 3), wts.at[3:6, 0:rows, 0:hpart])
                wait(("dp", 3), wts.at[3:6, 0:rows, 0:hpart])
                for u in range(3, 6):
                    relay_p(u)
                    relay_q(u)

            ready(1)
            project([1], [0, 1, 2])
            out_rows(("op", 1), g_off + (1 - m) * zrows, hrows - zrows, to_p)
            for b in range(2):
                out_rows(("oq", b), g_off + b * hrows // 2, hrows // 2, to_q)
            def last_rows():
                out_rows(("oq", 2), f_off + m * zrows, hrows - zrows, to_q)

            extra(last_rows)
            tok_w(1)
            norm(1, 1, 1)
            ready(2)
            taps_load.wait()
            project([2], [2])
            project([0, 1, 2], [3])
            partner_gate(0, None)

            @extra
            def _():
                wait(("r", 3), wts.at[3:6, 0 : 2 * hrows, 0:hpart])
                project([3, 4, 5], [2, 3])
            partner_gate(1, None)
            def pass_on(b):
                block = orow(fq, g_off + b * hrows // 2, hrows // 2)
                wait(("oq", b), block)
                send(("orp",), block, block, to_p, 2)

            project([2], [0, 1])
            own_gate(0, ("ga",))
            pass_on(0)
            extra(lambda: project([3, 4], [0, 1]))
            wait(("op", 1), orow(fp, g_off, hrows - zrows))
            block = orow(fp, c_off, crows)
            send(("oz", 1), block, block, to_z, 4)
            extra(lambda: project([5], [0, 1]))
            own_gate(1, ("ga",))
            pl.when(tp == 0)(lambda: forward(("gz", 0, None), None, part + hpart, hpart, ("ga",)))
            pl.when(tp == 1)(lambda: forward(("gz", 0, None), None, part, part, ("ga",)))
            pass_on(1)
            pl.when(tp == 1)(last_rows)
            block = orow(fq, c_off, crows)
            send(("oz", 1), block, block, to_z, 4)
            forward(("gz", 1, None), None, 2 * part, part, ("gb",))
            ow_load.wait()
            take_other(("ga",), None, 2)
            take_other(("gb",), None, 1)
            wait(("oz", 2), outw.at[0 : 2 * zrows])
            odd = lax.rem(fs, 2)
            mix(None, [krow(fs, 0), krow(fp, 0), krow(fd + m * (fq - fd), 0),
                       krow(fs + odd * (fx - fs), hrows)], True, False)
            for h in range(2):
                forward(("gz", 2, h), h, 3 * part, part, ("gc", h))
            wait(("oq", 2), orow(fq, f_off, hrows - zrows))
            late = [krow(fq, f_off), krow(fp + m * (fd - fp), hrows), krow(fx + odd * (fs - fx), hrows)]
            take_other(("gc", 0), 0, 1)
            mix(0, late, False, False)
            wait(("orp",), orow(fd, g_off, hrows))
            mix(0, [krow(fd, g_off)], False, True)
            take_other(("gc", 1), 1, 1)
            mix(1, late + [krow(fd, g_off)], False, True)
            pl.when(tp == 0)(lambda: wait_sent(0, wts.at[0:6, 0 : 9 * hrows // 2]))
            pl.when(tp == 1)(lambda: wait_sent(0, wts.at[0:3, 0 : 6 * hrows]))
            wait_sent(1, tok.at[0])
            wait_sent(2, outw.at[0 : 7 * hrows - 2 * zrows])
            pl.when(tp == 0)(lambda: wait_sent(3, gat.at[:, 0 : 11 * hpart]))
            pl.when(tp == 1)(lambda: wait_sent(3, gat.at[:, 0 : 10 * hpart]))
            wait_sent(4, outw.at[0 : 2 * crows])

    @pl.when(inner_chip == 1)
    def _():
        program(True)

    @pl.when(inner_chip == 0)
    def _():
        program(False)

    assert len(cross) <= CROSS


def paired(tokens, norm_gain, outer_weight, inner_weight, value_weight, conv_taps, out_weight):
    _, seq, width = tokens.shape
    rows, cols = outer_weight.shape
    part = cols // PARTS
    anyspace = pl.BlockSpec(memory_space=pltpu.HBM)
    vmem = pl.BlockSpec(memory_space=pltpu.VMEM)
    out = pl.pallas_call(
        kernel,
        out_shape=pltpu.VMEM((seq, cols), BF16),
        in_specs=[anyspace] * 7,
        out_specs=vmem,
        scratch_shapes=[
            pltpu.VMEM((1, width), F32),
            pltpu.VMEM(conv_taps.shape, F32),
            pltpu.VMEM((2, seq, width), BF16),
            pltpu.VMEM((2 * seq, width), BF16),
            pltpu.VMEM((3 * (PARTS - 1), width, part), BF16),
            pltpu.VMEM((width, cols), BF16),
            pltpu.VMEM((3, PARTS - 1, 2, seq + PAD, part), BF16),
            pltpu.VMEM((seq, width), BF16),
            pltpu.VMEM((PARTS - 1, seq, part), BF16),
            pltpu.VMEM((seq, cols), F32),
            pltpu.SemaphoreType.DMA((5,)),
            pltpu.SemaphoreType.DMA((COPIES,)),
            pltpu.SemaphoreType.DMA((5,)),
        ],
        compiler_params=pltpu.CompilerParams(
            collective_id=0, has_side_effects=True, vmem_limit_bytes=58 * 1024 * 1024
        ),
        name="mixer",
    )(
        tokens.reshape(seq, width), norm_gain.reshape(1, width), outer_weight, inner_weight,
        value_weight, conv_taps, out_weight,
    )
    return out.reshape(1, seq, cols)


def solution(mesh):
    shape = dict(mesh.shape)

    def local(tokens, *rest):
        rows, cols = rest[1].shape
        fits = (
            shape["fs"] == 4 and shape["tp"] == 2 and shape["rep"] == 4
            and tokens.shape[0] == 1 and tokens.shape[1] % 256 == 0
            and rows % 512 == 0 and cols == 2 * rows and rest[4].shape[0] <= 9
        )
        return (paired if fits else plain)(tokens, *rest)

    in_specs = (
        P(("rep", "fs"), None, None),
        P(),
        P("fs", "tp"),
        P("fs", "tp"),
        P("fs", "tp"),
        P(),
        P("fs", "tp"),
    )
    out_specs = P(("rep", "fs"), None, "tp")
    return jax.shard_map(local, mesh=mesh, in_specs=in_specs, out_specs=out_specs, check_vma=False)
```
